32 devices in a mesh: grp: 2 (over y), sp: 4 (over z), tp: 4 (over x, core).
Axes of the slice: x: 2, y: 2, z: 4, core: 2. Of those that a mesh axis runs over, the one named last changes fastest.
Arguments:
- gate_in: bfloat16 [4096, 1536], P(('grp', 'sp'), 'tp'), parts along dimension 0, may hold values from -6 to 6
- mult_in: bfloat16 [4096, 1536], P(('grp', 'sp'), 'tp'), parts along dimension 0, may hold values from -6 to 6
- value_in: bfloat16 [4096, 1536], P(('grp', 'sp'), 'tp'), parts along dimension 0, may hold values from -6 to 6
- doc_ids: int32 [4096], P(('grp', 'sp')), parts along dimension 0, may hold values from 0 to 1, never falling along the last dimension, each value on 1 to 1536 neighbouring positions
- conv_taps: bfloat16 [3, 1536], P(None, 'tp'), may hold values from -3 to 3
- out_proj: bfloat16 [1536, 2048], P('tp'), may hold values from -0.15625 to 0.15625
- resid: bfloat16 [4096, 2048], P(('grp', 'sp', 'tp')), parts along dimension 0, may hold values from -6 to 6
- norm1_gain: float32 [2048], replicated, may hold values from 0.1 to 1.9
- norm1_bias: float32 [2048], replicated, may hold values from -1.5 to 1.5
- expert_ids: int32 [4096, 2], P(('grp', 'sp', 'tp')), parts along dimension 0, may hold values from 0 to 3, all different within a row; in each aligned block of 128 rows (0 to 127, 128 to 255, ...) at most 80 rows name the same one
- expert_wts: float32 [4096, 2], P(('grp', 'sp', 'tp')), parts along dimension 0, may hold values from 0.1 to 1
- w_gate: bfloat16 [4, 2048, 3072], P('sp', None, 'tp'), may hold values from -0.125 to 0.125
- w_up: bfloat16 [4, 2048, 3072], P('sp', None, 'tp'), may hold values from -0.125 to 0.125
- w_down: bfloat16 [4, 3072, 2048], P('sp', 'tp'), may hold values from -0.21582031 to 0.21582031
- norm2_gain: float32 [2048], replicated, may hold values from 0.1 to 1.9
- norm2_bias: float32 [2048], replicated, may hold values from -1.5 to 1.5
Outputs:
- result: bfloat16 [4096, 2048], P(('grp', 'sp', 'tp')), parts along dimension 0
The draws below stay inside these ranges and needn't reach their ends.
There are 2 independent parts, one for each index of `grp`. The reference program is written for one: setup_inputs(seed, part) draws one part's arguments, and reference() takes and returns one part's arrays. A program takes and returns all parts, laid end to end along the dimension named above; an argument that names none is the same for every part. Nothing has to cross between parts.
Inputs may be any that keep to these rules, and one draw needn't show every extreme that they name: `doc_ids`: never falling along the sequence; each document has 1 to 1536 positions and one has exactly 1536. `expert_ids`: each row names 2 different experts. Among the rows of one device no expert is named more than 80 times, and in some device's rows some expert is named exactly 80 times.
All inputs are finite; a program needn't handle non-finite values.
Results may differ from the reference program's by a relative error of at most 0.0095.
Values may be sent and summed in bfloat16 or wider, within the bound.
A program may use at most 128 MiB of HBM per device.

```python
import math
import jax
import jax.numpy as jnp
import numpy as np
from jax import lax

D = 2048
D_CONV = 1536
FF_E = 3072
KW = 3
TOPK = 2
TOK_DEV = 128
TOKENS = 2048
EXPERTS = 4
CAP = 80
DOCS = 2
DOC_MOST = 1536
N_TP = 4


def block_levels(rng, extent, shards, smallest, largest):
    loudness, own = 1.0, jax.random.fold_in(rng, 6)
    for dim, shards_of in shards:
        steps = jnp.exp(jax.random.uniform(jax.random.fold_in(own, dim), (shards_of,), jnp.float32, smallest / len(shards), largest / len(shards)))
        loudness = loudness * jnp.repeat(steps, extent[dim] // shards_of).reshape([-1 if axis == dim else 1 for axis in range(len(extent))])
    return loudness


def profile(number_of, total, reach, skew):
    weights = [(1 << 20) // math.isqrt(grade ** skew) + 1 for grade in range(2, number_of + 1)]
    surplus, counts = total - reach - (number_of - 1), [1] * (number_of - 1)
    while surplus > 0:
        candidates = [i for i in range(number_of - 1) if counts[i] < reach]
        whole, left = sum([weights[i] for i in candidates]), surplus
        for i in candidates:
            extra = min(reach - counts[i], max(1, left * weights[i] // whole), surplus)
            counts[i] = counts[i] + extra
            surplus = surplus - extra
    return np.array([reach] + counts)


def ragged_sizes(rng, number_of, total, limit, lean):
    if number_of == 2:
        one = jax.random.randint(rng, (), max(1, total - limit), min(limit, total - 1) + 1)
        return jnp.stack([one, total - one])
    tallies = jnp.asarray(profile(number_of, total, limit, lean), jnp.int32)
    twos = (number_of - 1) // 2
    donor, receiver = tallies[1:1 + 2 * twos:2], tallies[2:2 + 2 * twos:2]
    room = jnp.minimum(donor - 1, limit - receiver)
    moved = jax.random.randint(jax.random.fold_in(rng, 1), (twos,), 0, 1 << 20) % (room + 1)
    tallies = tallies.at[1:1 + 2 * twos:2].set(donor - moved).at[2:2 + 2 * twos:2].set(receiver + moved)
    return tallies[jax.random.permutation(jax.random.fold_in(rng, 2), number_of)]


def routed_block(key, own, number, rows, number_of, top, most, lean):
    ranking = jax.random.permutation(key, number_of)
    packed, ordinary = shares(number_of, rows * top, most, lean, True), shares(number_of, rows * top, most, lean, False)
    places = jnp.arange(number_of)

    def named(lengths, offset_by):
        used = int((lengths > 0).sum())
        fixed = max(1, used // 4)
        passed = fixed + (places - fixed + offset_by * (used - fixed)) % max(1, number_of - fixed)
        return jnp.zeros((number_of,), jnp.int32).at[ranking[jnp.where(places < fixed, places, passed)]].set(jnp.asarray(lengths, jnp.int32))

    lengths = jnp.where(number % 4 == 0, named(packed, number // 4), named(ordinary, number - number // 4 - 1))
    mixed = jax.random.permutation(jax.random.fold_in(own, 3), number_of)
    donor, receiver = mixed[0:number_of // 2 * 2:2], mixed[1:number_of // 2 * 2:2]
    slack = jnp.minimum(lengths[donor] - 1, most - lengths[receiver]) // 2
    slack = jnp.where((donor == ranking[0]) | (receiver == ranking[0]) | (lengths[receiver] == 0), 0, jnp.maximum(slack, 0))
    passed = jax.random.randint(jax.random.fold_in(own, 4), (number_of // 2,), 0, 1 << 20) % (slack + 1)
    lengths = lengths.at[donor].add(-passed).at[receiver].add(passed)
    items = jnp.searchsorted(jnp.cumsum(lengths), jnp.arange(rows * top), side="right").astype(jnp.int32)
    table = items.reshape(top, rows).T
    table = table[jax.random.permutation(jax.random.fold_in(own, 1), rows)]
    offset_by = jax.random.randint(jax.random.fold_in(own, 2), (rows, 1), 0, top)
    return jnp.take_along_axis(table, (jnp.arange(top)[None, :] + offset_by) % top, axis=1)


def shares(number_of, total, limit, skew, full):
    portions = [(1 << 20) // math.isqrt(grade ** skew) + 1 for grade in range(1, number_of + 1)]
    largest = limit if full else min(limit, max(-(-total // number_of), total * portions[0] // sum(portions)))
    least = 1 if total - largest >= number_of - 1 else 0
    counts, surplus = [largest] + [least] * (number_of - 1), total - largest - least * (number_of - 1)
    while surplus > 0:
        candidates = [i for i in range(1, number_of) if counts[i] < largest] or [i for i in range(1, number_of) if counts[i] < limit]
        whole, left = sum([portions[i] for i in candidates]), surplus
        for i in candidates:
            more = min(limit - counts[i], max(1, left * portions[i] // whole), surplus)
            counts[i] = counts[i] + more
            surplus = surplus - more
    return np.array(counts)


def scatter_about(own_key, extent, width, most, split=(), kind=jnp.bfloat16):
    result = jax.random.normal(own_key, extent, jnp.float32) * width
    if len(split) > 0:
        result = block_levels(own_key, extent, split, -0.22, 0.18) * result
    return jnp.clip(result, min=-most, max=most).astype(kind)


def setup_inputs(seed: int = 0, part: int = 0) -> dict:
    streams_of = jax.random.split(jax.random.key(seed), 17)
    part_keys = jax.random.split(jax.random.fold_in(streams_of[16], part), 17)
    gate_in = scatter_about(part_keys[0], (TOKENS, D_CONV), 1.0, 6.0, ((0, 4), (1, 4)))
    mult_in = scatter_about(part_keys[1], (TOKENS, D_CONV), 1.0, 6.0, ((0, 4), (1, 4)))
    value_in = scatter_about(part_keys[2], (TOKENS, D_CONV), 1.0, 6.0, ((0, 4), (1, 4)))
    doc_ids = jnp.searchsorted(jnp.cumsum(ragged_sizes(part_keys[3], DOCS, TOKENS, DOC_MOST, 1)), jnp.arange(TOKENS), side="right").astype(jnp.int32)
    conv_taps = scatter_about(streams_of[4], (KW, D_CONV), 0.577, 3.0, ((1, 4),))
    out_proj = scatter_about(streams_of[5], (D_CONV, D), D_CONV ** -0.5, 0.15625, ((0, 4),))
    resid = scatter_about(part_keys[6], (TOKENS, D), 1.0, 6.0, ((0, 16),))
    norm1_gain = jnp.clip(1.0 + 0.18 * jax.random.normal(streams_of[7], (D,), jnp.float32), 0.1, 1.9)
    norm1_bias = scatter_about(streams_of[8], (D,), 0.3, 1.5, (), jnp.float32)
    expert_ids_keys = jax.random.split(jax.random.fold_in(part_keys[9], 1), TOKENS // TOK_DEV)
    expert_ids_turns = jax.random.permutation(jax.random.fold_in(part_keys[9], 3), TOKENS // TOK_DEV)
    expert_ids = jax.vmap(lambda own, number: routed_block(jax.random.fold_in(part_keys[9], 2), own, number, TOK_DEV, EXPERTS, TOPK, CAP, 2))(expert_ids_keys, expert_ids_turns).reshape((TOKENS, TOPK))
    expert_wts = jnp.clip(0.1 + 0.9 * jax.random.uniform(part_keys[10], (TOKENS, TOPK), jnp.float32) ** block_levels(part_keys[10], (TOKENS, TOPK), ((0, 16),), -0.2, 0.2), 0.1, 1.0)
    w_gate = scatter_about(streams_of[11], (EXPERTS, D, FF_E), D ** -0.5, 0.125, ((0, 4), (2, 4)))
    w_up = scatter_about(streams_of[12], (EXPERTS, D, FF_E), D ** -0.5, 0.125, ((0, 4), (2, 4)))
    w_down = scatter_about(streams_of[13], (EXPERTS, FF_E, D), (2.0 / FF_E ** 0.5), 0.21582031, ((0, 4), (1, 4)))
    norm2_gain = jnp.clip(1.0 + 0.18 * jax.random.normal(streams_of[14], (D,), jnp.float32), 0.1, 1.9)
    norm2_bias = scatter_about(streams_of[15], (D,), 0.3, 1.5, (), jnp.float32)
    return dict(gate_in=gate_in, mult_in=mult_in, value_in=value_in, doc_ids=doc_ids, conv_taps=conv_taps, out_proj=out_proj, resid=resid, norm1_gain=norm1_gain, norm1_bias=norm1_bias, expert_ids=expert_ids, expert_wts=expert_wts, w_gate=w_gate, w_up=w_up, w_down=w_down, norm2_gain=norm2_gain, norm2_bias=norm2_bias)


residual_scale = 2.0 ** 0.5
norm_eps = 1e-05

def layer_norm(pre, gain, bias):
    center = pre - lax.optimization_barrier(jnp.mean(pre, axis=-1, keepdims=True))
    spread = lax.optimization_barrier(jnp.mean(center * center, axis=-1, keepdims=True))
    return center * lax.rsqrt(spread + norm_eps) * gain + bias

def reference(gate_in, mult_in, value_in, doc_ids, conv_taps, out_proj, resid, norm1_gain, norm1_bias, expert_ids, expert_wts, w_gate, w_up, w_down, norm2_gain, norm2_bias):
    tap_weights = conv_taps.astype(jnp.float32)
    product = mult_in.astype(jnp.float32) * value_in.astype(jnp.float32)
    row_count = product.shape[0]
    padded = jnp.pad(product, ((KW - 1, 0), (0, 0)))
    doc_padded = jnp.concatenate([jnp.full((KW - 1,), -1, jnp.int32), doc_ids.astype(jnp.int32)])
    filtered = jnp.zeros_like(product)
    for tap_index in range(KW):
        shifted = padded[tap_index:tap_index + row_count]
        same_doc = (doc_padded[tap_index:tap_index + row_count] == doc_ids)[:, None]
        filtered = filtered + tap_weights[tap_index] * jnp.where(same_doc, shifted, 0.0)
    mixed_heads = (gate_in.astype(jnp.float32) * filtered).astype(jnp.bfloat16)
    mixed = jnp.dot(mixed_heads, out_proj, preferred_element_type=jnp.float32)
    hidden_one = layer_norm(residual_scale * resid.astype(jnp.float32) + mixed, norm1_gain, norm1_bias).astype(jnp.bfloat16)
    flat_ids = expert_ids.reshape(-1)
    flat_wts = expert_wts.reshape(-1)
    most_rows = CAP * (TOKENS // TOK_DEV)
    part_width = FF_E // N_TP

    def one_expert(moe, inputs):
        gate_w, up_w, down_w, number = inputs
        chosen = flat_ids == number
        picks = jnp.nonzero(chosen, size=most_rows, fill_value=0)[0].astype(jnp.int32)
        live = jnp.arange(most_rows, dtype=jnp.int32) < jnp.sum(chosen.astype(jnp.int32))
        rows = (picks // TOPK).astype(jnp.int32)
        inputs_rows = hidden_one[rows]
        gate_act = jnp.dot(inputs_rows, gate_w, preferred_element_type=jnp.float32)
        up_act = jnp.dot(inputs_rows, up_w, preferred_element_type=jnp.float32)
        hid = (jax.nn.silu(gate_act) * up_act).astype(jnp.bfloat16)
        total = jnp.zeros((most_rows, D), jnp.float32)
        for part in range(N_TP):
            piece = jnp.dot(hid[:, part * part_width:(part + 1) * part_width], down_w[part * part_width:(part + 1) * part_width], preferred_element_type=jnp.float32).astype(jnp.bfloat16)
            total = total + lax.optimization_barrier(piece).astype(jnp.float32)
        expert_out = lax.optimization_barrier(total.astype(jnp.bfloat16)).astype(jnp.float32)
        weight = jnp.where(live, flat_wts[picks], 0.0)
        return (moe.at[rows].add(weight[:, None] * expert_out), None)
    moe_start = jnp.zeros((row_count, D), jnp.float32)
    numbers = jnp.arange(EXPERTS, dtype=jnp.int32)
    moe, _ = lax.scan(one_expert, moe_start, (w_gate, w_up, w_down, numbers))
    return layer_norm(residual_scale * hidden_one.astype(jnp.float32) + moe, norm2_gain, norm2_bias).astype(jnp.bfloat16)
```

```python
import functools

import jax
import jax.numpy as jnp
from jax import lax
from jax.experimental import pallas as pl
from jax.experimental.pallas import tpu as pltpu
from jax.sharding import PartitionSpec as P

residual_scale = 2.0**0.5
norm_eps = 1e-05
MESH = pl.DeviceIdType.MESH
f32, bf16 = jnp.float32, jnp.bfloat16
CHUNKS = 4


def layer_norm(pre, gain, bias):
    center = pre - jnp.mean(pre, axis=-1, keepdims=True)
    spread = jnp.mean(center * center, axis=-1, keepdims=True)
    return center * lax.rsqrt(spread + norm_eps) * gain + bias


def remote(src, dst, send, recv, **where):
    return pltpu.make_async_remote_copy(
        src_ref=src, dst_ref=dst, send_sem=send, recv_sem=recv, device_id=where, device_id_type=MESH
    )


def kernel(
    experts, slots, piece,
    gate_h, mult_h, value_h, docs_h, taps_h, proj_h, resid_h, gain1_h, bias1_h, ids_h, wts_h,
    w_gate_h, w_up_h, w_down_h, gain2_h, bias2_h,
    out_h,
    gate, mult, value, docs, taps, proj, resid, gain1, bias1, ids, wts, w_gate, w_up, w_down, gain2, bias2,
    edge_m, edge_v, ext, ext_docs, heads,
    send1, got1, send2, got2, own, hidden, out, slot_of, weight_of, onehot, picks_l, picks,
    rows_l, part_l, sum_in_l, sum_send_l, cross_l, done_l,
    packed, rows, part, hid, sum_in, sum_send, cross_in, done_out, back,
    local, outs, edge_s, edge_r, mix_s, mix_r,
    ls, lr, r2ls, r2lr,
    zs, zr, xs, xr, bs, br, cs, cr, r1s, r1r, r2s, r2r, r3s, r3r,
):
    s, t = lax.axis_index("sp"), lax.axis_index("tp")
    hi, lo = t // 2, t % 2
    sib, far = hi * 2 + (1 - lo), (1 - hi) * 2 + lo
    count, model = resid.shape
    length, channels = mult.shape
    taps_n = taps.shape[0]
    top = ids.shape[0]
    others = experts - 1
    pieces = slots // piece

    def load(i, a, b):
        return pltpu.make_async_copy(a, b, local.at[i])

    pairs = [
        (mult_h, mult), (value_h, value), (docs_h, docs.at[:, 128 : 128 + length]), (taps_h, taps), (gate_h, gate),
        (proj_h, proj), (resid_h, resid), (gain1_h, gain1), (bias1_h, bias1), (ids_h, ids), (wts_h, wts),
        (w_gate_h, w_gate), (w_up_h, w_up), (w_down_h, w_down), (gain2_h, gain2), (bias2_h, bias2),
    ]
    loads = [load(i, a, b) for i, (a, b) in enumerate(pairs)]
    for c in loads[:11]:
        c.start()

    barrier = pltpu.get_barrier_semaphore()

    def greet(d, _):
        pl.semaphore_signal(barrier, inc=1, device_id={"sp": (s + d) % experts}, device_id_type=MESH)
        return 0

    lax.fori_loop(1, experts, greet, 0)
    pl.semaphore_signal(barrier, inc=1, device_id={"tp": sib}, device_id_type=MESH)
    pl.semaphore_signal(barrier, inc=1, device_id={"tp": far}, device_id_type=MESH)
    for c in loads[:3]:
        c.wait()
    pl.semaphore_wait(barrier, experts + 1)

    nxt = (s + 1) % experts
    edges = [
        remote(mult.at[pl.ds(length - 16, 16)], edge_m, edge_s.at[0], edge_r.at[0], sp=nxt),
        remote(value.at[pl.ds(length - 16, 16)], edge_v, edge_s.at[1], edge_r.at[1], sp=nxt),
        remote(docs.at[:, pl.ds(length, 128)], docs.at[:, pl.ds(0, 128)], edge_s.at[2], edge_r.at[2], sp=nxt),
    ]

    @pl.when(s < experts - 1)
    def _():
        for c in edges:
            c.start()

    for c in loads[11:]:
        c.start()

    ones = jnp.ones((128, 128), bf16)
    row_no = lax.broadcasted_iota(jnp.int32, (128, 128), 0)
    lane_no = lax.broadcasted_iota(jnp.int32, (128, 128), 1)

    def column(line, shift, height):
        spread = jnp.where(row_no[:height] + shift == lane_no[:height], line.astype(f32), 0.0)
        return jnp.dot(spread.astype(bf16), ones, preferred_element_type=f32)

    for r in range(0, length, 128):
        ext[8 + r : 8 + r + 128, :] = mult[r : r + 128, :].astype(f32) * value[r : r + 128, :].astype(f32)
        ext_docs[8 + r : 8 + r + 128, :] = column(docs[:, 128 + r : 256 + r], 0, 128)
    ext[0:8, :] = jnp.zeros((8, channels), f32)
    ext_docs[0:8, :] = jnp.full((8, 128), -1.0, f32)
    for c in loads[3:5]:
        c.wait()

    def convolve(r, height):
        now = ext_docs[8 + r : 8 + r + height, :]
        same = [ext_docs[8 + r - b : 8 + r - b + height, :] == now for b in range(1, taps_n)]
        for c in range(0, channels, 128):
            tap = taps[:, c : c + 128].astype(f32)
            acc = tap[taps_n - 1 :] * ext[8 + r : 8 + r + height, c : c + 128]
            for b in range(1, taps_n):
                moved = ext[8 + r - b : 8 + r - b + height, c : c + 128]
                acc = acc + tap[taps_n - 1 - b : taps_n - b] * jnp.where(same[b - 1], moved, 0.0)
            heads[r : r + height, c : c + 128] = (gate[r : r + height, c : c + 128].astype(f32) * acc).astype(bf16)

    for r in range(0, length, 64):
        convolve(r, 64)

    @pl.when(s > 0)
    def _():
        for c in edges:
            c.wait_recv()
        ext[0:8, :] = (edge_m[...].astype(f32) * edge_v[...].astype(f32))[8:16, :]
        ext_docs[0:8, :] = column(docs[:, 0:128], 120, 8)
        convolve(0, 16)

    loads[5].wait()
    wide = 512

    def projected(number, n):
        return jnp.dot(
            heads[pl.ds(pl.multiple_of(number * count, count), count), :], proj[:, n : n + wide],
            preferred_element_type=f32,
        )

    step = count // CHUNKS
    near = [
        remote(send1.at[0, pl.ds(j * step, step)], got1.at[0, pl.ds(j * step, step)], mix_s.at[j], mix_r.at[j], tp=sib)
        for j in range(CHUNKS)
    ]
    over = [
        remote(send2.at[pl.ds(j * step, step)], got2.at[pl.ds(j * step, step)], mix_s.at[CHUNKS + j], mix_r.at[CHUNKS + j], tp=far)
        for j in range(CHUNKS)
    ]
    last = remote(send1.at[1], got1.at[1], mix_s.at[2 * CHUNKS], mix_r.at[2 * CHUNKS], tp=sib)
    for n in range(0, model, wide):
        send1[0, :, n : n + wide] = projected((1 - hi) * 2 + (1 - lo), n).astype(bf16)
    for c in near:
        c.start()
    for n in range(0, model, wide):
        own[:, n : n + wide] = projected((1 - hi) * 2 + lo, n)
    for j in range(CHUNKS):
        q = slice(j * step, (j + 1) * step)
        near[j].wait_recv()
        send2[q, :] = (own[q, :] + got1[0, q, :].astype(f32)).astype(bf16)
        over[j].start()
    for n in range(0, model, wide):
        send1[1, :, n : n + wide] = projected(hi * 2 + (1 - lo), n).astype(bf16)
    last.start()
    loads[6].wait()
    for n in range(0, model, wide):
        own[:, n : n + wide] = projected(t, n) + residual_scale * resid[:, n : n + wide].astype(f32)

    for c in loads[7:11]:
        c.wait()
    padded = slot_of.shape[0]
    expert_no = lax.broadcasted_iota(jnp.int32, (padded, count), 0)
    chosen = jnp.zeros((padded, count), f32)
    weight = jnp.zeros((padded, count), f32)
    for k in range(top):
        same = ids[k : k + 1, :] == expert_no
        chosen = chosen + jnp.where(same, 1.0, 0.0)
        weight = weight + jnp.where(same, wts[k : k + 1, :], 0.0)
    before = lax.broadcasted_iota(jnp.int32, (count, count), 0) < lax.broadcasted_iota(
        jnp.int32, (count, count), 1
    )
    rank = jnp.dot(chosen.astype(bf16), jnp.where(before, 1.0, 0.0).astype(bf16), preferred_element_type=f32)
    slot_of[...] = jnp.where(chosen > 0.5, rank, -1.0)
    weight_of[...] = weight
    slot_no = lax.broadcasted_iota(jnp.int32, (slots, count), 0).astype(f32)

    def choose(d, put):
        e = (s + d) % experts
        selected = slot_no == slot_of[pl.ds(e, 1), :]
        onehot[pl.ds(pl.multiple_of(d * slots, 16), slots), :] = jnp.where(selected, 1.0, 0.0).astype(bf16)
        pick = jnp.where(selected, weight_of[pl.ds(e, 1), :], 0.0)
        high = pick.astype(bf16)
        put(high, (pick - high.astype(f32)).astype(bf16))

    def put_local(high, low):
        picks_l[:, 0:count] = high
        picks_l[:, count : 2 * count] = low

    choose(0, put_local)

    def choose_step(d, _):
        def put(high, low):
            for k in range(pieces):
                picks[k, d - 1, :, 0:count] = high[k * piece : (k + 1) * piece, :]
                picks[k, d - 1, :, count : 2 * count] = low[k * piece : (k + 1) * piece, :]

        choose(d, put)
        return 0

    lax.fori_loop(1, experts, choose_step, 0)

    last.wait_recv()
    for n in range(0, model, wide):
        own[:, n : n + wide] = own[:, n : n + wide] + got1[1, :, n : n + wide].astype(f32)
    for j in range(CHUNKS):
        over[j].wait_recv()
        q = slice(j * step, (j + 1) * step)
        hidden[q, :] = layer_norm(own[q, :] + got2[q, :].astype(f32), gain1[...], bias1[...]).astype(bf16)

    mine, other = lo * 2 + hi, lo * 2 + 1 - hi

    def z_out(k, d):
        return remote(packed.at[k, d - 1], rows.at[k, mine, d - 1], zs.at[k, d - 1], zr.at[k, d - 1], sp=(s + d) % experts)

    def x_copy(k):
        block = rows.at[k, mine]
        return remote(block, block, xs.at[k], xr.at[k], tp=far)

    def b_copy(k):
        block = rows.at[k, mine]
        return remote(block, block, bs.at[k], br.at[k], tp=sib)

    def c_copy(k):
        block = rows.at[k, other]
        return remote(block, block, cs.at[k], cr.at[k], tp=sib)

    def r1_copy(k):
        return remote(part.at[k, pl.ds((1 - lo) * 2, 2)], sum_in.at[k], r1s.at[k], r1r.at[k], tp=sib)

    def r2_copy(k):
        return remote(sum_send.at[k], cross_in.at[k], r2s.at[k], r2r.at[k], tp=far)

    def r3_copy(k, d):
        return remote(done_out.at[k, d - 1], back.at[k, d - 1], r3s.at[k, d - 1], r3r.at[k, d - 1], sp=(s - d + experts) % experts)

    x_l = remote(rows_l.at[mine], rows_l.at[mine], ls.at[0], lr.at[0], tp=far)
    b_l = remote(rows_l.at[mine], rows_l.at[mine], ls.at[1], lr.at[1], tp=sib)
    c_l = remote(rows_l.at[other], rows_l.at[other], ls.at[2], lr.at[2], tp=sib)
    r1_l = remote(part_l.at[pl.ds((1 - lo) * 2, 2)], sum_in_l, ls.at[3], lr.at[3], tp=sib)

    def r2_l(j):
        q = pl.ds(j * piece, piece)
        return remote(sum_send_l.at[q], cross_l.at[q], r2ls.at[j], r2lr.at[j], tp=far)

    def each(count_of, run):
        def step(i, _):
            run(i)
            return 0

        lax.fori_loop(0, count_of, step, 0)

    def across(run):
        def step(d, _):
            run(d)
            return 0

        lax.fori_loop(1, experts, step, 0)

    for n in range(0, model, wide):
        y = jnp.dot(onehot[0:slots, :], hidden[:, n : n + wide], preferred_element_type=f32)
        rows_l[mine, :, n : n + wide] = y.astype(bf16)
    x_l.start()
    b_l.start()
    for n in range(0, model, wide):
        y = jnp.dot(onehot[slots:, :], hidden[:, n : n + wide], preferred_element_type=f32).astype(bf16)
        for d in range(others):
            for k in range(pieces):
                r = d * slots + k * piece
                packed[k, d, :, n : n + wide] = y[r : r + piece, :]
    each(pieces, lambda k: across(lambda d: z_out(k, d).start()))
    for n in range(0, model, wide):
        own[:, n : n + wide] = residual_scale * hidden[:, n : n + wide].astype(f32)
    for c in loads[11:]:
        c.wait()

    wide_f = 256

    def ffn(size, take, put):
        for n in range(0, w_gate.shape[1], wide_f):
            x = take()
            g = jnp.dot(x, w_gate[:, n : n + wide_f], preferred_element_type=f32)
            u = jnp.dot(x, w_up[:, n : n + wide_f], preferred_element_type=f32)
            hid[0:size, n : n + wide_f] = (jax.nn.silu(g) * u).astype(bf16)
        for n in range(0, model, wide_f):
            y = jnp.dot(hid[0:size, :], w_down[:, n : n + wide_f], preferred_element_type=f32)
            put(n, y.astype(bf16))

    group = 4 if 4 * others * piece <= 512 else 1
    size = group * others * piece

    def experts_of(k):
        def run(m, _):
            block = pl.ds(m * group, group)

            def put(n, y):
                part[k, block, :, :, n : n + wide_f] = y.reshape(group, others, piece, wide_f)

            ffn(size, lambda: rows[k, block].reshape(size, model), put)
            return 0

        if group == 4:
            run(0, 0)
        else:
            lax.fori_loop(0, 4 // group, run, 0)

    def put_l(n, y):
        part_l[:, :, n : n + wide_f] = y.reshape(4, slots, wide_f)

    def arrive(k):
        across(lambda d: z_out(k, d).wait_recv())
        x_copy(k).start()
        b_copy(k).start()

    def combine(pick, value_of):
        dims = (((0,), (0,)), ((), ()))
        for n in range(0, model, wide):
            y = lax.dot_general(pick, value_of(n), dims, preferred_element_type=f32)
            own[:, n : n + wide] = own[:, n : n + wide] + y[0:count, :] + y[count:, :]

    def give_back(k):
        across(lambda d: r3_copy(k, d).wait_recv())
        combine(
            picks[k].reshape(others * piece, 2 * count),
            lambda n: back[k, :, :, n : n + wide].reshape(others * piece, wide),
        )

    arrive(0)
    x_l.wait_recv()
    c_l.start()
    b_l.wait_recv()
    c_l.wait_recv()
    ffn(4 * slots, lambda: rows_l[...].reshape(4 * slots, model), put_l)
    r1_l.start()

    def turn(d, _):
        @pl.when(d < pieces)
        def _():
            arrive(d)

        @pl.when(d == 1)
        def _():
            r1_l.wait_recv()

            def add(j):
                q = pl.ds(pl.multiple_of(j * piece, 16), piece)
                sum_send_l[q, :] = (part_l[other, q, :].astype(f32) + sum_in_l[1 - hi, q, :].astype(f32)).astype(bf16)

            each(pieces, add)

        @pl.when(jnp.logical_and(d >= 2, d < pieces + 2))
        def _():
            k = d - 2
            r1_copy(k).wait_recv()

            def add(j):
                total = part[k, other, j].astype(f32) + sum_in[k, 1 - hi, j].astype(f32)
                sum_send[k, j] = total.astype(bf16)

            each(others, add)
            r2_copy(k).start()

        @pl.when(d == pieces + 1)
        def _():
            each(pieces, lambda j: r2_l(j).start())

        @pl.when(d < pieces + 1)
        def _():
            k = d - 1
            x_copy(k).wait_recv()
            c_copy(k).start()
            b_copy(k).wait_recv()
            c_copy(k).wait_recv()
            experts_of(k)
            r1_copy(k).start()

        @pl.when(d >= 3)
        def _():
            k = d - 3
            r2_copy(k).wait_recv()

            def add(j):
                total = part[k, mine, j].astype(f32) + sum_in[k, hi, j].astype(f32) + cross_in[k, j].astype(f32)
                done_out[k, j] = total.astype(bf16)

            each(others, add)
            across(lambda i: r3_copy(k, i).start())

        return 0

    lax.fori_loop(1, pieces + 3, turn, 0)
    for k in range(max(pieces - 2, 0)):
        give_back(k)

    def add_l(j):
        q = pl.ds(pl.multiple_of(j * piece, 16), piece)
        r2_l(j).wait_recv()
        total = part_l[mine, q, :].astype(f32) + sum_in_l[hi, q, :].astype(f32) + cross_l[q, :].astype(f32)
        done_l[q, :] = total.astype(bf16)

    each(pieces, add_l)
    combine(picks_l[...], lambda n: done_l[:, n : n + wide])
    for k in range(max(pieces - 2, 0), pieces):
        give_back(k)

    finals = []
    for j in range(CHUNKS):
        q = slice(j * step, (j + 1) * step)
        out[q, :] = layer_norm(own[q, :], gain2[...], bias2[...]).astype(bf16)
        c = pltpu.make_async_copy(out.at[pl.ds(j * step, step)], out_h.at[pl.ds(j * step, step)], outs.at[j])
        c.start()
        finals.append(c)

    @pl.when(s < experts - 1)
    def _():
        for c in edges:
            c.wait_send()

    for c in near + over + [last, x_l, b_l, c_l, r1_l]:
        c.wait_send()

    def drain(k):
        for c in (x_copy, b_copy, c_copy, r1_copy, r2_copy, r2_l):
            c(k).wait_send()
        across(lambda d: z_out(k, d).wait_send())
        across(lambda d: r3_copy(k, d).wait_send())

    each(pieces, drain)
    for c in finals:
        c.wait()


def shards(
    gate_in, mult_in, value_in, doc_ids, conv_taps, out_proj, resid, norm1_gain, norm1_bias,
    expert_ids, expert_wts, w_gate, w_up, w_down, norm2_gain, norm2_bias,
):
    experts, parts = lax.axis_size("sp"), lax.axis_size("tp")
    assert parts == 4
    length, channels = mult_in.shape
    count, model = resid.shape
    top = expert_ids.shape[1]
    units = w_gate.shape[2]
    capacity = 5 * count * top // (4 * experts)
    piece = 16
    pieces = -(-capacity // piece)
    slots = pieces * piece
    padded = max(8, experts)
    others = experts - 1
    hbm = pl.BlockSpec(memory_space=pl.ANY)
    V = pltpu.VMEM
    sems = pltpu.SemaphoreType.DMA
    blocks = (pieces, others, piece, model)
    routed = (pieces, 4, others, piece, model)
    batch = 4 * others * piece if 4 * others * piece <= 512 else others * piece
    batch = max(batch, 4 * slots)
    many, each_way = sems((pieces,)), sems((pieces, others))
    return pl.pallas_call(
        functools.partial(kernel, experts, slots, piece),
        out_shape=jax.ShapeDtypeStruct((count, model), bf16),
        in_specs=[hbm] * 16,
        out_specs=hbm,
        scratch_shapes=[
            V((length, channels), bf16), V((length, channels), bf16), V((length, channels), bf16),
            V((1, length + 128), jnp.int32), V(conv_taps.shape, bf16), V((channels, model), bf16), V((count, model), bf16),
            V((1, model), f32), V((1, model), f32), V((top, count), jnp.int32), V((top, count), f32),
            V((model, units), bf16), V((model, units), bf16), V((units, model), bf16), V((1, model), f32), V((1, model), f32),
            V((16, channels), bf16), V((16, channels), bf16),
            V((length + 8, channels), f32), V((length + 8, 128), f32), V((length, channels), bf16),
            V((2, count, model), bf16), V((2, count, model), bf16), V((count, model), bf16),
            V((count, model), bf16), V((count, model), f32), V((count, model), bf16), V((count, model), bf16),
            V((padded, count), f32), V((padded, count), f32), V((experts * slots, count), bf16),
            V((slots, 2 * count), bf16), V((pieces, others, piece, 2 * count), bf16),
            V((4, slots, model), bf16), V((4, slots, model), bf16), V((2, slots, model), bf16),
            V((slots, model), bf16), V((slots, model), bf16), V((slots, model), bf16),
            V(blocks, bf16), V(routed, bf16), V(routed, bf16), V((batch, units), bf16),
            V((pieces, 2, others, piece, model), bf16), V(blocks, bf16), V(blocks, bf16), V(blocks, bf16),
            V(blocks, bf16),
            sems((16,)), sems((CHUNKS,)), sems((3,)), sems((3,)), sems((2 * CHUNKS + 1,)), sems((2 * CHUNKS + 1,)),
            sems((4,)), sems((4,)), many, many,
            each_way, each_way, many, many, many, many, many, many,
            many, many, many, many, each_way, each_way,
        ],
        compiler_params=pltpu.CompilerParams(
            collective_id=0, has_side_effects=True, vmem_limit_bytes=62 * 2**20
        ),
    )(
        gate_in, mult_in, value_in, doc_ids[None], conv_taps, out_proj, resid,
        norm1_gain[None], norm1_bias[None], expert_ids.T, expert_wts.T,
        w_gate[0], w_up[0], w_down[0], norm2_gain[None], norm2_bias[None],
    )


def solution(mesh):
    placed = (
        P(("grp", "sp"), "tp"),
        P(("grp", "sp"), "tp"),
        P(("grp", "sp"), "tp"),
        P(("grp", "sp")),
        P(None, "tp"),
        P("tp", None),
        P(("grp", "sp", "tp"), None),
        P(),
        P(),
        P(("grp", "sp", "tp"), None),
        P(("grp", "sp", "tp"), None),
        P("sp", None, "tp"),
        P("sp", None, "tp"),
        P("sp", "tp", None),
        P(),
        P(),
    )
    return jax.shard_map(
        shards, mesh=mesh, in_specs=placed, out_specs=P(("grp", "sp", "tp"), None), check_vma=False
    )
```

```python
import functools

import jax
import jax.numpy as jnp
from jax import lax
from jax.experimental import pallas as pl
from jax.experimental.pallas import tpu as pltpu
from jax.sharding import PartitionSpec as P

residual_scale = 2.0**0.5
norm_eps = 1e-05
MESH = pl.DeviceIdType.MESH
f32, bf16 = jnp.float32, jnp.bfloat16
CHUNKS = 4


def layer_norm(pre, gain, bias):
    center = pre - jnp.mean(pre, axis=-1, keepdims=True)
    spread = jnp.mean(center * center, axis=-1, keepdims=True)
    return center * lax.rsqrt(spread + norm_eps) * gain + bias


def remote(src, dst, send, recv, **where):
    return pltpu.make_async_remote_copy(
        src_ref=src, dst_ref=dst, send_sem=send, recv_sem=recv, device_id=where, device_id_type=MESH
    )


def kernel(
    experts, slots, piece,
    gate_h, mult_h, value_h, docs_h, taps_h, proj_h, resid_h, gain1_h, bias1_h, ids_h, wts_h,
    w_gate_h, w_up_h, w_down_h, gain2_h, bias2_h,
    out_h,
    gate, mult, value, docs, taps, proj, resid, gain1, bias1, ids, wts, w_gate, w_up, w_down, gain2, bias2,
    edge_m, edge_v, ext, ext_docs, heads,
    send1, got1, send2, got2, own, hidden, hidden_far, out, ids_far, wts_far,
    slot_of, weight_of, onehot_n, onehot, picks_n, picks,
    rows_n, part_n, pack_n, sum_in_n, total_n, near_back, dense_send, dense_in,
    packed, rows, part, hid, sum_in, sum_send, cross_in, done_out, back,
    local, outs, edge_s, edge_r, mix_s, mix_r, swap_s, swap_r, dense_s, dense_r,
    lbs, lbr, ns, nr, nbs, nbr, n1s, n1r, rns, rnr, des, der,
    zs, zr, xs, xr, bs, br, cs, cr, r1s, r1r, r2s, r2r, r3s, r3r,
):
    s, t = lax.axis_index("sp"), lax.axis_index("tp")
    hi, lo = t // 2, t % 2
    sib, far = hi * 2 + (1 - lo), (1 - hi) * 2 + lo
    count, model = resid.shape
    length, channels = mult.shape
    taps_n = taps.shape[0]
    top = ids.shape[0]
    others = experts - 2
    pieces = slots // piece
    parity = s % 2
    base = s - parity
    near = base + 1 - parity

    def load(i, a, b):
        return pltpu.make_async_copy(a, b, local.at[i])

    pairs = [
        (mult_h, mult), (value_h, value), (docs_h, docs.at[:, 128 : 128 + length]), (taps_h, taps), (gate_h, gate),
        (proj_h, proj), (resid_h, resid), (gain1_h, gain1), (bias1_h, bias1), (ids_h, ids), (wts_h, wts),
        (w_gate_h, w_gate), (w_up_h, w_up), (w_down_h, w_down), (gain2_h, gain2), (bias2_h, bias2),
    ]
    loads = [load(i, a, b) for i, (a, b) in enumerate(pairs)]
    for c in loads[:11]:
        c.start()

    barrier = pltpu.get_barrier_semaphore()

    def greet(d, _):
        pl.semaphore_signal(barrier, inc=1, device_id={"sp": (s + d) % experts}, device_id_type=MESH)
        return 0

    lax.fori_loop(1, experts, greet, 0)
    pl.semaphore_signal(barrier, inc=1, device_id={"tp": sib}, device_id_type=MESH)
    pl.semaphore_signal(barrier, inc=1, device_id={"tp": far}, device_id_type=MESH)
    for c in loads[:3]:
        c.wait()
    pl.semaphore_wait(barrier, experts + 1)

    nxt = (s + 1) % experts
    edges = [
        remote(mult.at[pl.ds(length - 16, 16)], edge_m, edge_s.at[0], edge_r.at[0], sp=nxt),
        remote(value.at[pl.ds(length - 16, 16)], edge_v, edge_s.at[1], edge_r.at[1], sp=nxt),
        remote(docs.at[:, pl.ds(length, 128)], docs.at[:, pl.ds(0, 128)], edge_s.at[2], edge_r.at[2], sp=nxt),
    ]

    @pl.when(s < experts - 1)
    def _():
        for c in edges:
            c.start()

    for c in loads[11:]:
        c.start()

    ones = jnp.ones((128, 128), bf16)
    row_no = lax.broadcasted_iota(jnp.int32, (128, 128), 0)
    lane_no = lax.broadcasted_iota(jnp.int32, (128, 128), 1)

    def column(line, shift, height):
        spread = jnp.where(row_no[:height] + shift == lane_no[:height], line.astype(f32), 0.0)
        return jnp.dot(spread.astype(bf16), ones, preferred_element_type=f32)

    for r in range(0, length, 128):
        ext[8 + r : 8 + r + 128, :] = mult[r : r + 128, :].astype(f32) * value[r : r + 128, :].astype(f32)
        ext_docs[8 + r : 8 + r + 128, :] = column(docs[:, 128 + r : 256 + r], 0, 128)
    ext[0:8, :] = jnp.zeros((8, channels), f32)
    ext_docs[0:8, :] = jnp.full((8, 128), -1.0, f32)
    for c in loads[3:5]:
        c.wait()

    def convolve(r, height):
        now = ext_docs[8 + r : 8 + r + height, :]
        same = [ext_docs[8 + r - b : 8 + r - b + height, :] == now for b in range(1, taps_n)]
        for c in range(0, channels, 128):
            tap = taps[:, c : c + 128].astype(f32)
            acc = tap[taps_n - 1 :] * ext[8 + r : 8 + r + height, c : c + 128]
            for b in range(1, taps_n):
                moved = ext[8 + r - b : 8 + r - b + height, c : c + 128]
                acc = acc + tap[taps_n - 1 - b : taps_n - b] * jnp.where(same[b - 1], moved, 0.0)
            heads[r : r + height, c : c + 128] = (gate[r : r + height, c : c + 128].astype(f32) * acc).astype(bf16)

    for r in range(0, length, 64):
        convolve(r, 64)

    @pl.when(s > 0)
    def _():
        for c in edges:
            c.wait_recv()
        ext[0:8, :] = (edge_m[...].astype(f32) * edge_v[...].astype(f32))[8:16, :]
        ext_docs[0:8, :] = column(docs[:, 0:128], 120, 8)
        convolve(0, 16)

    for c in loads[7:11]:
        c.wait()
    swaps = [
        remote(ids, ids_far, swap_s.at[0], swap_r.at[0], tp=far),
        remote(wts, wts_far, swap_s.at[1], swap_r.at[1], tp=far),
    ]
    for c in swaps:
        c.start()
    loads[5].wait()
    wide = 512

    def projected(number, n):
        return jnp.dot(
            heads[pl.ds(pl.multiple_of(number * count, count), count), :], proj[:, n : n + wide],
            preferred_element_type=f32,
        )

    step = count // CHUNKS
    beside = [
        remote(send1.at[0, pl.ds(j * step, step)], got1.at[0, pl.ds(j * step, step)], mix_s.at[j], mix_r.at[j], tp=sib)
        for j in range(CHUNKS)
    ]
    over = [
        remote(send2.at[pl.ds(j * step, step)], got2.at[pl.ds(j * step, step)], mix_s.at[CHUNKS + j], mix_r.at[CHUNKS + j], tp=far)
        for j in range(CHUNKS)
    ]
    last = remote(send1.at[1], got1.at[1], mix_s.at[2 * CHUNKS], mix_r.at[2 * CHUNKS], tp=sib)
    dense = [
        remote(hidden.at[pl.ds(j * step, step)], hidden_far.at[pl.ds(j * step, step)], dense_s.at[j], dense_r.at[j], tp=far)
        for j in range(CHUNKS)
    ]
    for n in range(0, model, wide):
        send1[0, :, n : n + wide] = projected((1 - hi) * 2 + (1 - lo), n).astype(bf16)
    for c in beside:
        c.start()
    for n in range(0, model, wide):
        own[:, n : n + wide] = projected((1 - hi) * 2 + lo, n)
    for j in range(CHUNKS):
        q = slice(j * step, (j + 1) * step)
        beside[j].wait_recv()
        send2[q, :] = (own[q, :] + got1[0, q, :].astype(f32)).astype(bf16)
        over[j].start()
    for n in range(0, model, wide):
        send1[1, :, n : n + wide] = projected(hi * 2 + (1 - lo), n).astype(bf16)
    last.start()
    loads[6].wait()
    for n in range(0, model, wide):
        own[:, n : n + wide] = projected(t, n) + residual_scale * resid[:, n : n + wide].astype(f32)
    last.wait_recv()
    for n in range(0, model, wide):
        own[:, n : n + wide] = own[:, n : n + wide] + got1[1, :, n : n + wide].astype(f32)

    padded = slot_of.shape[1]
    expert_no = lax.broadcasted_iota(jnp.int32, (padded, count), 0)
    token_no = lax.broadcasted_iota(jnp.int32, (padded, count), 1)
    before = lax.broadcasted_iota(jnp.int32, (count, count), 0) < lax.broadcasted_iota(
        jnp.int32, (count, count), 1
    )
    slot_no = lax.broadcasted_iota(jnp.int32, (slots, count), 0).astype(f32)
    ready = [max(0, slots - (count - (j + 1) * step)) // piece for j in range(CHUNKS)]

    def choose(side, e, put):
        selected = slot_no == slot_of[side, pl.ds(e, 1), :]
        pick = jnp.where(selected, weight_of[side, pl.ds(e, 1), :], 0.0)
        high = pick.astype(bf16)
        put(jnp.where(selected, 1.0, 0.0).astype(bf16), high, (pick - high.astype(f32)).astype(bf16))

    def route(side, own_side, its_ids, its_wts):
        chosen = jnp.zeros((padded, count), f32)
        weight = jnp.zeros((padded, count), f32)
        for k in range(top):
            same = its_ids[k : k + 1, :] == expert_no
            chosen = chosen + jnp.where(same, 1.0, 0.0)
            weight = weight + jnp.where(same, its_wts[k : k + 1, :], 0.0)
        rank = jnp.dot(chosen.astype(bf16), jnp.where(before, 1.0, 0.0).astype(bf16), preferred_element_type=f32)
        slot, placed, open_ = jnp.full((padded, count), -1.0, f32), jnp.zeros((padded, 1), f32), 0
        for j in range(CHUNKS):
            seen = jnp.where(token_no < (j + 1) * step, chosen, 0.0)
            upto = jnp.minimum(jnp.sum(seen, axis=1, keepdims=True), placed + float(ready[j] * piece - open_))
            here = jnp.logical_and(rank >= placed, rank < upto)
            slot = jnp.where(here, rank - placed + float(open_), slot)
            placed, open_ = upto, ready[j] * piece
        slot_of[side] = jnp.where(chosen > 0.5, slot, -1.0)
        weight_of[side] = weight
        for n, e in enumerate((s, near)):
            def put(one, high, low):
                if own_side:
                    for k in range(pieces):
                        onehot[k, others + n] = one[k * piece : (k + 1) * piece, :]
                else:
                    onehot_n[n * slots : (n + 1) * slots, :] = one
                picks_n[side, n * slots : (n + 1) * slots, 0:count] = high
                picks_n[side, n * slots : (n + 1) * slots, count : 2 * count] = low

            choose(side, e, put)

    route(hi, True, ids, wts)

    def choose_step(i, _):
        def put(one, high, low):
            for k in range(pieces):
                onehot[k, i] = one[k * piece : (k + 1) * piece, :]
                picks[k, i, :, 0:count] = high[k * piece : (k + 1) * piece, :]
                picks[k, i, :, count : 2 * count] = low[k * piece : (k + 1) * piece, :]

        choose(hi, (base + 2 + i) % experts, put)
        return 0

    lax.fori_loop(0, others, choose_step, 0)
    for c in swaps:
        c.wait_recv()
    route(1 - hi, False, ids_far, wts_far)

    hidden[...] = jnp.zeros((count, model), bf16)

    mine, other = lo * 2 + hi, lo * 2 + 1 - hi

    def z_out(k, i):
        j = 2 * (i // 2) + parity
        return remote(packed.at[k, i], rows.at[k, mine, j], zs.at[k, i], zr.at[k, j], sp=(base + 2 + i) % experts)

    def z_got(k, j):
        return remote(packed.at[k, j], rows.at[k, mine, j], zs.at[k, j], zr.at[k, j], sp=near)

    def x_copy(k):
        block = rows.at[k, mine]
        return remote(block, block, xs.at[k], xr.at[k], tp=far)

    def b_copy(k):
        block = rows.at[k, mine]
        return remote(block, block, bs.at[k], br.at[k], tp=sib)

    def c_copy(k):
        block = rows.at[k, other]
        return remote(block, block, cs.at[k], cr.at[k], tp=sib)

    def r1_copy(k):
        return remote(part.at[k, pl.ds((1 - lo) * 2, 2)], sum_in.at[k], r1s.at[k], r1r.at[k], tp=sib)

    def r2_copy(k):
        return remote(sum_send.at[k], cross_in.at[k], r2s.at[k], r2r.at[k], tp=far)

    def r3_copy(k, j):
        i = 2 * (j // 2) + parity
        to = (base - 2 - 2 * (j // 2) + j % 2 + experts) % experts
        return remote(done_out.at[k, j], back.at[k, i], r3s.at[k, j], r3r.at[k, i], sp=to)

    def r3_got(k, i):
        return remote(done_out.at[k, i], back.at[k, i], r3s.at[k, i], r3r.at[k, i], sp=near)

    def local_copy(h):
        block = rows_n.at[0, h, lo]
        return remote(block, block, lbs.at[h], lbr.at[h], tp=sib)

    def near_far():
        return remote(pack_n.at[1 - hi], rows_n.at[1, 1 - hi, lo], ns.at[CHUNKS], nr.at[CHUNKS], sp=near)

    def near_own(j, first, stop):
        q = pl.ds(first * piece, (stop - first) * piece)
        return remote(pack_n.at[hi, q], rows_n.at[1, hi, lo, q], ns.at[j], nr.at[j], sp=near)

    stages, begun = [], 0
    for j in range(CHUNKS):
        if ready[j] > begun:
            stages.append((j, begun, ready[j]))
            begun = ready[j]
    held = max(pieces - 2, 1)

    def near_share(h):
        block = rows_n.at[1, h, lo]
        return remote(block, block, nbs.at[h], nbr.at[h], tp=sib)

    def near_sum(n, h):
        return remote(part_n.at[n, h, 1 - lo], sum_in_n.at[n, h], n1s.at[n, h], n1r.at[n, h], tp=sib)

    def near_return(h, c):
        return remote(total_n.at[h, c], near_back.at[h, c, 1], rns.at[h, c], rnr.at[h, c], sp=near)

    def dense_copy(c):
        return remote(dense_send.at[c], dense_in.at[c], des.at[c], der.at[c], tp=far)

    def each(count_of, run):
        def step(i, _):
            run(i)
            return 0

        lax.fori_loop(0, count_of, step, 0)

    def across(run):
        each(others, run)

    for j in range(CHUNKS):
        over[j].wait_recv()
        q = slice(j * step, (j + 1) * step)
        hidden[q, :] = layer_norm(own[q, :] + got2[q, :].astype(f32), gain1[...], bias1[...]).astype(bf16)
        dense[j].start()
        for number, first, stop in stages:
            if number != j:
                continue
            span = stop - first
            q = slice(first * piece, stop * piece)
            for n in range(0, model, wide):
                y = jnp.dot(
                    onehot[first:stop].reshape(span * experts * piece, count), hidden[:, n : n + wide],
                    preferred_element_type=f32,
                ).astype(bf16).reshape(span, experts, piece, wide)
                packed[first:stop, :, :, n : n + wide] = y[:, :others]
                rows_n[0, hi, lo, q, n : n + wide] = y[:, others].reshape(span * piece, wide)
                pack_n[hi, q, n : n + wide] = y[:, others + 1].reshape(span * piece, wide)
            near_own(j, first, stop).start()
            for k in range(first, min(stop, held)):
                across(lambda i: z_out(k, i).start())

    local_copy(hi).start()
    for n in range(0, model, wide):
        own[:, n : n + wide] = residual_scale * hidden[:, n : n + wide].astype(f32)
    for c in loads[11:]:
        c.wait()

    wide_f = 256

    def ffn(size, take, put):
        for n in range(0, w_gate.shape[1], wide_f):
            x = take()
            g = jnp.dot(x, w_gate[:, n : n + wide_f], preferred_element_type=f32)
            u = jnp.dot(x, w_up[:, n : n + wide_f], preferred_element_type=f32)
            hid[0:size, n : n + wide_f] = (jax.nn.silu(g) * u).astype(bf16)
        for n in range(0, model, wide_f):
            y = jnp.dot(hid[0:size, :], w_down[:, n : n + wide_f], preferred_element_type=f32)
            put(n, y.astype(bf16))

    group = 4 if 4 * others * piece <= 512 else 1
    size = group * others * piece

    def experts_of(k):
        def run(m, _):
            block = pl.ds(m * group, group)

            def put(n, y):
                part[k, block, :, :, n : n + wide_f] = y.reshape(group, others, piece, wide_f)

            ffn(size, lambda: rows[k, block].reshape(size, model), put)
            return 0

        if group == 4:
            run(0, 0)
        else:
            lax.fori_loop(0, 4 // group, run, 0)

    def arrive(k):
        across(lambda j: z_got(k, j).wait_recv())
        x_copy(k).start()
        b_copy(k).start()

    half = model // 2

    def near_total(n, h, put):
        near_sum(n, h).wait_recv()
        for c in range(2):
            q = slice(c * half, (c + 1) * half)
            total = part_n[n, h, lo, :, q].astype(f32) + sum_in_n[n, h, :, q].astype(f32)
            put(c, total.astype(bf16))

    def near_expert(h):
        near_share(h).wait_recv()

        def put(n, y):
            part_n[1, h, :, :, n : n + wide_f] = y.reshape(2, slots, wide_f)

        ffn(2 * slots, lambda: rows_n[1, h].reshape(2 * slots, model), put)
        near_sum(1, h).start()

    def near_home(h):
        def put(c, y):
            total_n[h, c] = y
            near_return(h, c).start()

        near_total(1, h, put)

    dims = (((0,), (0,)), ((), ()))

    def near_combine(h, c, put):
        near_return(h, c).wait_recv()
        for n in range(0, half, wide):
            y = lax.dot_general(
                picks_n[h], near_back[h, c, :, :, n : n + wide].reshape(2 * slots, wide), dims, preferred_element_type=f32
            )
            put(n, y[0:count, :] + y[count:, :])

    def far_combine(c):
        def put(n, y):
            dense_send[c, :, n : n + wide] = y.astype(bf16)

        near_combine(1 - hi, c, put)
        dense_copy(c).start()

    def give_back(k):
        across(lambda i: r3_got(k, i).wait_recv())
        for n in range(0, model, wide):
            y = lax.dot_general(
                picks[k].reshape(others * piece, 2 * count), back[k, :, :, n : n + wide].reshape(others * piece, wide),
                dims, preferred_element_type=f32,
            )
            own[:, n : n + wide] = own[:, n : n + wide] + y[0:count, :] + y[count:, :]

    arrive(0)
    for c in dense:
        c.wait_recv()
    for n in range(0, model, wide):
        y = jnp.dot(onehot_n[...], hidden_far[:, n : n + wide], preferred_element_type=f32).astype(bf16)
        rows_n[0, 1 - hi, lo, :, n : n + wide] = y[0:slots, :]
        pack_n[1 - hi, :, n : n + wide] = y[slots:, :]
    near_far().start()
    for k in range(held, pieces):
        across(lambda i: z_out(k, i).start())
    local_copy(1 - hi).start()
    if pieces > 1:
        arrive(1)

    def put_local(n, y):
        part_n[0, :, :, :, n : n + wide_f] = y.reshape(2, 2, slots, wide_f)

    def local_expert():
        local_copy(hi).wait_recv()
        local_copy(1 - hi).wait_recv()
        ffn(4 * slots, lambda: rows_n[0].reshape(4 * slots, model), put_local)
        near_sum(0, 0).start()
        near_sum(0, 1).start()

    steps = {"share": 3, "expert": 3, "home": 4, "local": 4, "total": 5, "expert_own": 5, "home_own": 6, "cross": 6, "cross2": 6}
    turns = max(pieces + 3, max(steps.values()) + 1)

    def turn(d, _):
        def at(name, run):
            @pl.when(d == steps[name])
            def _():
                run()

        @pl.when(d < pieces + 1)
        def _():
            k = d - 1
            x_copy(k).wait_recv()
            c_copy(k).start()

        @pl.when(jnp.logical_and(d >= 2, d < pieces + 2))
        def _():
            k = d - 2
            r1_copy(k).wait_recv()

            def add(j):
                total = part[k, other, j].astype(f32) + sum_in[k, 1 - hi, j].astype(f32)
                sum_send[k, j] = total.astype(bf16)

            across(add)
            r2_copy(k).start()

        at("home", lambda: near_home(1 - hi))
        at("home_own", lambda: near_home(hi))
        @pl.when(jnp.logical_and(d >= 3, d < pieces + 3))
        def _():
            k = d - 3
            r2_copy(k).wait_recv()

            def add(j):
                total = part[k, mine, j].astype(f32) + sum_in[k, hi, j].astype(f32) + cross_in[k, j].astype(f32)
                done_out[k, j] = total.astype(bf16)

            across(add)
            across(lambda j: r3_copy(k, j).start())

        if pieces > 2:
            @pl.when(d == 1)
            def _():
                arrive(2)

        def share():
            near_far().wait_recv()
            near_share(1 - hi).start()
            for stage in stages:
                near_own(*stage).wait_recv()
            near_share(hi).start()

        at("share", share)

        @pl.when(d < pieces + 1)
        def _():
            k = d - 1
            b_copy(k).wait_recv()
            c_copy(k).wait_recv()
            experts_of(k)
            r1_copy(k).start()

        @pl.when(jnp.logical_and(d >= 2, d < pieces - 1))
        def _():
            arrive(d + 1)

        def total_local():
            for h in range(2):
                def put(c, y):
                    near_back[h, c, 0] = y

                near_total(0, h, put)

        at("expert", lambda: near_expert(1 - hi))
        at("local", local_expert)
        at("total", total_local)
        at("expert_own", lambda: near_expert(hi))
        at("cross", lambda: far_combine(0))
        at("cross2", lambda: far_combine(1))
        return 0

    lax.fori_loop(1, turns, turn, 0)
    for k in range(max(pieces - 1, 0)):
        give_back(k)
    for c in range(2):
        def put(n, y):
            q = slice(c * half + n, c * half + n + wide)
            own[:, q] = own[:, q] + y

        near_combine(hi, c, put)
    for k in range(max(pieces - 1, 0), pieces):
        give_back(k)
    for c in range(2):
        dense_copy(c).wait_recv()

    finals = []
    for j in range(CHUNKS):
        q = slice(j * step, (j + 1) * step)
        crossed = jnp.concatenate([dense_in[0, q, :], dense_in[1, q, :]], axis=1).astype(f32)
        out[q, :] = layer_norm(own[q, :] + crossed, gain2[...], bias2[...]).astype(bf16)
        c = pltpu.make_async_copy(out.at[pl.ds(j * step, step)], out_h.at[pl.ds(j * step, step)], outs.at[j])
        c.start()
        finals.append(c)

    @pl.when(s < experts - 1)
    def _():
        for c in edges:
            c.wait_send()

    for c in beside + over + dense + swaps + [last, near_far()] + [near_own(*stage) for stage in stages]:
        c.wait_send()
    for h in range(2):
        for c in (local_copy(h), near_share(h), near_sum(0, h), near_sum(1, h), near_return(h, 0), near_return(h, 1), dense_copy(h)):
            c.wait_send()

    def drain(k):
        for c in (x_copy, b_copy, c_copy, r1_copy, r2_copy):
            c(k).wait_send()
        across(lambda i: z_out(k, i).wait_send())
        across(lambda j: r3_copy(k, j).wait_send())

    each(pieces, drain)
    for c in finals:
        c.wait()


def shards(
    gate_in, mult_in, value_in, doc_ids, conv_taps, out_proj, resid, norm1_gain, norm1_bias,
    expert_ids, expert_wts, w_gate, w_up, w_down, norm2_gain, norm2_bias,
):
    experts, parts = lax.axis_size("sp"), lax.axis_size("tp")
    assert parts == 4
    length, channels = mult_in.shape
    count, model = resid.shape
    top = expert_ids.shape[1]
    units = w_gate.shape[2]
    capacity = 5 * count * top // (4 * experts)
    piece = 16
    pieces = -(-capacity // piece)
    slots = pieces * piece
    padded = max(8, experts)
    others = experts - 2
    assert experts >= 4 and experts % 2 == 0
    hbm = pl.BlockSpec(memory_space=pl.ANY)
    V = pltpu.VMEM
    sems = pltpu.SemaphoreType.DMA
    blocks = (pieces, others, piece, model)
    routed = (pieces, 4, others, piece, model)
    batch = 4 * others * piece if 4 * others * piece <= 512 else others * piece
    batch = max(batch, 4 * slots)
    many, each_way = sems((pieces,)), sems((pieces, others))
    two, four = sems((2,)), sems((2, 2))
    return pl.pallas_call(
        functools.partial(kernel, experts, slots, piece),
        out_shape=jax.ShapeDtypeStruct((count, model), bf16),
        in_specs=[hbm] * 16,
        out_specs=hbm,
        scratch_shapes=[
            V((length, channels), bf16), V((length, channels), bf16), V((length, channels), bf16),
            V((1, length + 128), jnp.int32), V(conv_taps.shape, bf16), V((channels, model), bf16), V((count, model), bf16),
            V((1, model), f32), V((1, model), f32), V((top, count), jnp.int32), V((top, count), f32),
            V((model, units), bf16), V((model, units), bf16), V((units, model), bf16), V((1, model), f32), V((1, model), f32),
            V((16, channels), bf16), V((16, channels), bf16),
            V((length + 8, channels), f32), V((length + 8, 128), f32), V((length, channels), bf16),
            V((2, count, model), bf16), V((2, count, model), bf16), V((count, model), bf16), V((count, model), bf16),
            V((count, model), f32), V((count, model), bf16), V((count, model), bf16), V((count, model), bf16),
            V((top, count), jnp.int32), V((top, count), f32),
            V((2, padded, count), f32), V((2, padded, count), f32), V((2 * slots, count), bf16),
            V((pieces, experts, piece, count), bf16), V((2, 2 * slots, 2 * count), bf16), V((pieces, others, piece, 2 * count), bf16),
            V((2, 2, 2, slots, model), bf16), V((2, 2, 2, slots, model), bf16), V((2, slots, model), bf16),
            V((2, 2, slots, model), bf16), V((2, 2, slots, model // 2), bf16), V((2, 2, 2, slots, model // 2), bf16),
            V((2, count, model // 2), bf16), V((2, count, model // 2), bf16),
            V(blocks, bf16), V(routed, bf16), V(routed, bf16), V((batch, units), bf16),
            V((pieces, 2, others, piece, model), bf16), V(blocks, bf16), V(blocks, bf16), V(blocks, bf16),
            V(blocks, bf16),
            sems((16,)), sems((CHUNKS,)), sems((3,)), sems((3,)), sems((2 * CHUNKS + 1,)), sems((2 * CHUNKS + 1,)),
            two, two, sems((CHUNKS,)), sems((CHUNKS,)),
            two, two, sems((CHUNKS + 1,)), sems((CHUNKS + 1,)), two, two, four, four, four, four, two, two,
            each_way, each_way, many, many, many, many, many, many,
            many, many, many, many, each_way, each_way,
        ],
        compiler_params=pltpu.CompilerParams(
            collective_id=0, has_side_effects=True, vmem_limit_bytes=62 * 2**20
        ),
    )(
        gate_in, mult_in, value_in, doc_ids[None], conv_taps, out_proj, resid,
        norm1_gain[None], norm1_bias[None], expert_ids.T, expert_wts.T,
        w_gate[0], w_up[0], w_down[0], norm2_gain[None], norm2_bias[None],
    )


def solution(mesh):
    placed = (
        P(("grp", "sp"), "tp"),
        P(("grp", "sp"), "tp"),
        P(("grp", "sp"), "tp"),
        P(("grp", "sp")),
        P(None, "tp"),
        P("tp", None),
        P(("grp", "sp", "tp"), None),
        P(),
        P(),
        P(("grp", "sp", "tp"), None),
        P(("grp", "sp", "tp"), None),
        P("sp", None, "tp"),
        P("sp", None, "tp"),
        P("sp", "tp", None),
        P(),
        P(),
    )
    return jax.shard_map(
        shards, mesh=mesh, in_specs=placed, out_specs=P(("grp", "sp", "tp"), None), check_vma=False
    )
```

```python
import functools

import jax
import jax.numpy as jnp
from jax import lax
from jax.experimental import pallas as pl
from jax.experimental.pallas import tpu as pltpu
from jax.sharding import PartitionSpec as P

residual_scale = 2.0**0.5
norm_eps = 1e-05
MESH = pl.DeviceIdType.MESH
f32, bf16 = jnp.float32, jnp.bfloat16
CHUNKS = 4


def layer_norm(pre, gain, bias):
    center = pre - jnp.mean(pre, axis=-1, keepdims=True)
    spread = jnp.mean(center * center, axis=-1, keepdims=True)
    return center * lax.rsqrt(spread + norm_eps) * gain + bias


def remote(src, dst, send, recv, **where):
    return pltpu.make_async_remote_copy(
        src_ref=src, dst_ref=dst, send_sem=send, recv_sem=recv, device_id=where, device_id_type=MESH
    )


def kernel(
    experts, slots, piece,
    gate_h, mult_h, value_h, docs_h, taps_h, proj_h, resid_h, gain1_h, bias1_h, ids_h, wts_h,
    w_gate_h, w_up_h, w_down_h, gain2_h, bias2_h,
    out_h,
    gate, mult, value, docs, taps, proj, resid, gain1, bias1, ids, wts, w_gate, w_up, w_down, gain2, bias2,
    edge_m, edge_v, ext, ext_docs, heads,
    send1, got1, send2, got2, own, hidden, hidden_far, out, ids_far, wts_far,
    slot_of, weight_of, onehot_n, onehot, picks_n, picks,
    rows_n, part_n, pack_n, sum_in_n, total_n, near_back, dense_send, dense_in,
    packed, rows, part, hid, sum_in, sum_send, cross_in, done_out, back,
    local, outs, edge_s, edge_r, mix_s, mix_r, swap_s, swap_r, dense_s, dense_r,
    lbs, lbr, ns, nr, nbs, nbr, n1s, n1r, rns, rnr, des, der,
    zs, zr, xs, xr, bs, br, cs, cr, r1s, r1r, r2s, r2r, r3s, r3r,
):
    s, t = lax.axis_index("sp"), lax.axis_index("tp")
    hi, lo = t // 2, t % 2
    sib, far = hi * 2 + (1 - lo), (1 - hi) * 2 + lo
    count, model = resid.shape
    length, channels = mult.shape
    taps_n = taps.shape[0]
    top = ids.shape[0]
    others = experts - 2
    pieces = slots // piece
    parity = s % 2
    base = s - parity
    near = base + 1 - parity

    def load(i, a, b):
        return pltpu.make_async_copy(a, b, local.at[i])

    pairs = [
        (mult_h, mult), (value_h, value), (docs_h, docs.at[:, 128 : 128 + length]), (taps_h, taps), (gate_h, gate),
        (proj_h, proj), (resid_h, resid), (gain1_h, gain1), (bias1_h, bias1), (ids_h, ids), (wts_h, wts),
        (w_gate_h, w_gate), (w_up_h, w_up), (w_down_h, w_down), (gain2_h, gain2), (bias2_h, bias2),
    ]
    loads = [load(i, a, b) for i, (a, b) in enumerate(pairs)]
    for c in loads[:11]:
        c.start()

    barrier = pltpu.get_barrier_semaphore()

    def greet(d, _):
        pl.semaphore_signal(barrier, inc=1, device_id={"sp": (s + d) % experts}, device_id_type=MESH)
        return 0

    lax.fori_loop(1, experts, greet, 0)
    pl.semaphore_signal(barrier, inc=1, device_id={"tp": sib}, device_id_type=MESH)
    pl.semaphore_signal(barrier, inc=1, device_id={"tp": far}, device_id_type=MESH)
    for c in loads[:3]:
        c.wait()
    pl.semaphore_wait(barrier, experts + 1)

    nxt = (s + 1) % experts
    edges = [
        remote(mult.at[pl.ds(length - 16, 16)], edge_m, edge_s.at[0], edge_r.at[0], sp=nxt),
        remote(value.at[pl.ds(length - 16, 16)], edge_v, edge_s.at[1], edge_r.at[1], sp=nxt),
        remote(docs.at[:, pl.ds(length, 128)], docs.at[:, pl.ds(0, 128)], edge_s.at[2], edge_r.at[2], sp=nxt),
    ]

    @pl.when(s < experts - 1)
    def _():
        for c in edges:
            c.start()

    for c in loads[11:]:
        c.start()

    ones = jnp.ones((128, 128), bf16)
    row_no = lax.broadcasted_iota(jnp.int32, (128, 128), 0)
    lane_no = lax.broadcasted_iota(jnp.int32, (128, 128), 1)

    def column(line, shift, height):
        spread = jnp.where(row_no[:height] + shift == lane_no[:height], line.astype(f32), 0.0)
        return jnp.dot(spread.astype(bf16), ones, preferred_element_type=f32)

    for r in range(0, length, 128):
        ext[8 + r : 8 + r + 128, :] = mult[r : r + 128, :].astype(f32) * value[r : r + 128, :].astype(f32)
        ext_docs[8 + r : 8 + r + 128, :] = column(docs[:, 128 + r : 256 + r], 0, 128)
    ext[0:8, :] = jnp.zeros((8, channels), f32)
    ext_docs[0:8, :] = jnp.full((8, 128), -1.0, f32)
    for c in loads[3:5]:
        c.wait()

    def convolve(r, height):
        now = ext_docs[8 + r : 8 + r + height, :]
        same = [ext_docs[8 + r - b : 8 + r - b + height, :] == now for b in range(1, taps_n)]
        for c in range(0, channels, 128):
            tap = taps[:, c : c + 128].astype(f32)
            acc = tap[taps_n - 1 :] * ext[8 + r : 8 + r + height, c : c + 128]
            for b in range(1, taps_n):
                moved = ext[8 + r - b : 8 + r - b + height, c : c + 128]
                acc = acc + tap[taps_n - 1 - b : taps_n - b] * jnp.where(same[b - 1], moved, 0.0)
            heads[r : r + height, c : c + 128] = (gate[r : r + height, c : c + 128].astype(f32) * acc).astype(bf16)

    for r in range(0, length, 64):
        convolve(r, 64)

    @pl.when(s > 0)
    def _():
        for c in edges:
            c.wait_recv()
        ext[0:8, :] = (edge_m[...].astype(f32) * edge_v[...].astype(f32))[8:16, :]
        ext_docs[0:8, :] = column(docs[:, 0:128], 120, 8)
        convolve(0, 16)

    for c in loads[7:11]:
        c.wait()
    swaps = [
        remote(ids, ids_far, swap_s.at[0], swap_r.at[0], tp=far),
        remote(wts, wts_far, swap_s.at[1], swap_r.at[1], tp=far),
    ]
    for c in swaps:
        c.start()
    loads[5].wait()
    wide = 512

    def projected(number, n):
        return jnp.dot(
            heads[pl.ds(pl.multiple_of(number * count, count), count), :], proj[:, n : n + wide],
            preferred_element_type=f32,
        )

    step = count // CHUNKS
    beside = [
        remote(send1.at[0, pl.ds(j * step, step)], got1.at[0, pl.ds(j * step, step)], mix_s.at[j], mix_r.at[j], tp=sib)
        for j in range(CHUNKS)
    ]
    over = [
        remote(send2.at[pl.ds(j * step, step)], got2.at[pl.ds(j * step, step)], mix_s.at[CHUNKS + j], mix_r.at[CHUNKS + j], tp=far)
        for j in range(CHUNKS)
    ]
    last = remote(send1.at[1], got1.at[1], mix_s.at[2 * CHUNKS], mix_r.at[2 * CHUNKS], tp=sib)
    dense = [
        remote(hidden.at[pl.ds(j * step, step)], hidden_far.at[pl.ds(j * step, step)], dense_s.at[j], dense_r.at[j], tp=far)
        for j in range(CHUNKS)
    ]
    for n in range(0, model, wide):
        send1[0, :, n : n + wide] = projected((1 - hi) * 2 + (1 - lo), n).astype(bf16)
    for c in beside:
        c.start()
    for n in range(0, model, wide):
        own[:, n : n + wide] = projected((1 - hi) * 2 + lo, n)
    for j in range(CHUNKS):
        q = slice(j * step, (j + 1) * step)
        beside[j].wait_recv()
        send2[q, :] = (own[q, :] + got1[0, q, :].astype(f32)).astype(bf16)
        over[j].start()
    for n in range(0, model, wide):
        send1[1, :, n : n + wide] = projected(hi * 2 + (1 - lo), n).astype(bf16)
    last.start()
    loads[6].wait()
    for n in range(0, model, wide):
        own[:, n : n + wide] = projected(t, n) + residual_scale * resid[:, n : n + wide].astype(f32)
    last.wait_recv()
    for n in range(0, model, wide):
        own[:, n : n + wide] = own[:, n : n + wide] + got1[1, :, n : n + wide].astype(f32)

    padded = slot_of.shape[1]
    expert_no = lax.broadcasted_iota(jnp.int32, (padded, count), 0)
    token_no = lax.broadcasted_iota(jnp.int32, (padded, count), 1)
    before = lax.broadcasted_iota(jnp.int32, (count, count), 0) < lax.broadcasted_iota(
        jnp.int32, (count, count), 1
    )
    slot_no = lax.broadcasted_iota(jnp.int32, (slots, count), 0).astype(f32)
    ready = [max(0, slots - (count - (j + 1) * step)) // piece for j in range(CHUNKS)]

    def choose(side, e, put):
        selected = slot_no == slot_of[side, pl.ds(e, 1), :]
        pick = jnp.where(selected, weight_of[side, pl.ds(e, 1), :], 0.0)
        high = pick.astype(bf16)
        put(jnp.where(selected, 1.0, 0.0).astype(bf16), high, (pick - high.astype(f32)).astype(bf16))

    def route(side, own_side, its_ids, its_wts):
        chosen = jnp.zeros((padded, count), f32)
        weight = jnp.zeros((padded, count), f32)
        for k in range(top):
            same = its_ids[k : k + 1, :] == expert_no
            chosen = chosen + jnp.where(same, 1.0, 0.0)
            weight = weight + jnp.where(same, its_wts[k : k + 1, :], 0.0)
        rank = jnp.dot(chosen.astype(bf16), jnp.where(before, 1.0, 0.0).astype(bf16), preferred_element_type=f32)
        slot, placed, open_ = jnp.full((padded, count), -1.0, f32), jnp.zeros((padded, 1), f32), 0
        for j in range(CHUNKS):
            seen = jnp.where(token_no < (j + 1) * step, chosen, 0.0)
            upto = jnp.minimum(jnp.sum(seen, axis=1, keepdims=True), placed + float(ready[j] * piece - open_))
            here = jnp.logical_and(rank >= placed, rank < upto)
            slot = jnp.where(here, rank - placed + float(open_), slot)
            placed, open_ = upto, ready[j] * piece
        slot_of[side] = jnp.where(chosen > 0.5, slot, -1.0)
        weight_of[side] = weight
        for n, e in enumerate((s, near)):
            def put(one, high, low):
                if own_side:
                    for k in range(pieces):
                        onehot[k, others + n] = one[k * piece : (k + 1) * piece, :]
                else:
                    onehot_n[n * slots : (n + 1) * slots, :] = one
                picks_n[side, n * slots : (n + 1) * slots, 0:count] = high
                picks_n[side, n * slots : (n + 1) * slots, count : 2 * count] = low

            choose(side, e, put)

    route(hi, True, ids, wts)

    def choose_step(i, _):
        def put(one, high, low):
            for k in range(pieces):
                onehot[k, i] = one[k * piece : (k + 1) * piece, :]
                picks[k, i, :, 0:count] = high[k * piece : (k + 1) * piece, :]
                picks[k, i, :, count : 2 * count] = low[k * piece : (k + 1) * piece, :]

        choose(hi, (base + 2 + i) % experts, put)
        return 0

    lax.fori_loop(0, others, choose_step, 0)
    for c in swaps:
        c.wait_recv()
    route(1 - hi, False, ids_far, wts_far)

    hidden[...] = jnp.zeros((count, model), bf16)

    mine, other = lo * 2 + hi, lo * 2 + 1 - hi

    def z_out(k, i):
        j = 2 * (i // 2) + parity
        return remote(packed.at[k, i], rows.at[k, mine, j], zs.at[k, i], zr.at[k, j], sp=(base + 2 + i) % experts)

    def z_got(k, j):
        return remote(packed.at[k, j], rows.at[k, mine, j], zs.at[k, j], zr.at[k, j], sp=near)

    def x_copy(k):
        block = rows.at[k, mine]
        return remote(block, block, xs.at[k], xr.at[k], tp=far)

    def b_copy(k):
        block = rows.at[k, mine]
        return remote(block, block, bs.at[k], br.at[k], tp=sib)

    def c_copy(k):
        block = rows.at[k, other]
        return remote(block, block, cs.at[k], cr.at[k], tp=sib)

    def r1_copy(k):
        return remote(part.at[k, pl.ds((1 - lo) * 2, 2)], sum_in.at[k], r1s.at[k], r1r.at[k], tp=sib)

    def r2_copy(k):
        return remote(sum_send.at[k], cross_in.at[k], r2s.at[k], r2r.at[k], tp=far)

    def r3_copy(k, j):
        i = 2 * (j // 2) + parity
        to = (base - 2 - 2 * (j // 2) + j % 2 + experts) % experts
        return remote(done_out.at[k, j], back.at[k, i], r3s.at[k, j], r3r.at[k, i], sp=to)

    def r3_got(k, i):
        return remote(done_out.at[k, i], back.at[k, i], r3s.at[k, i], r3r.at[k, i], sp=near)

    def local_copy(h):
        block = rows_n.at[0, h, lo]
        return remote(block, block, lbs.at[h], lbr.at[h], tp=sib)

    def near_far():
        return remote(pack_n.at[1 - hi], rows_n.at[1, 1 - hi, lo], ns.at[CHUNKS], nr.at[CHUNKS], sp=near)

    def near_own(j, first, stop):
        q = pl.ds(first * piece, (stop - first) * piece)
        return remote(pack_n.at[hi, q], rows_n.at[1, hi, lo, q], ns.at[j], nr.at[j], sp=near)

    stages, begun = [], 0
    for j in range(CHUNKS):
        if ready[j] > begun:
            stages.append((j, begun, ready[j]))
            begun = ready[j]
    held = max(pieces - 1, 1)

    def near_share(h):
        block = rows_n.at[1, h, lo]
        return remote(block, block, nbs.at[h], nbr.at[h], tp=sib)

    def near_sum(n, h):
        return remote(part_n.at[n, h, 1 - lo], sum_in_n.at[n, h], n1s.at[n, h], n1r.at[n, h], tp=sib)

    def near_return(h, c):
        return remote(total_n.at[h, c], near_back.at[h, c, 1], rns.at[h, c], rnr.at[h, c], sp=near)

    def dense_copy(c):
        return remote(dense_send.at[c], dense_in.at[c], des.at[c], der.at[c], tp=far)

    def each(count_of, run):
        def step(i, _):
            run(i)
            return 0

        lax.fori_loop(0, count_of, step, 0)

    def across(run):
        each(others, run)

    for j in range(CHUNKS):
        over[j].wait_recv()
        q = slice(j * step, (j + 1) * step)
        hidden[q, :] = layer_norm(own[q, :] + got2[q, :].astype(f32), gain1[...], bias1[...]).astype(bf16)
        dense[j].start()
        for number, first, stop in stages:
            if number != j:
                continue
            span = stop - first
            q = slice(first * piece, stop * piece)
            for n in range(0, model, wide):
                y = jnp.dot(
                    onehot[first:stop].reshape(span * experts * piece, count), hidden[:, n : n + wide],
                    preferred_element_type=f32,
                ).astype(bf16).reshape(span, experts, piece, wide)
                packed[first:stop, :, :, n : n + wide] = y[:, :others]
                rows_n[0, hi, lo, q, n : n + wide] = y[:, others].reshape(span * piece, wide)
                pack_n[hi, q, n : n + wide] = y[:, others + 1].reshape(span * piece, wide)
            near_own(j, first, stop).start()
            for k in range(first, min(stop, held)):
                across(lambda i: z_out(k, i).start())

    local_copy(hi).start()
    for n in range(0, model, wide):
        own[:, n : n + wide] = residual_scale * hidden[:, n : n + wide].astype(f32)
    for c in loads[11:]:
        c.wait()

    wide_f = 256

    def ffn(size, take, put):
        for n in range(0, w_gate.shape[1], wide_f):
            x = take()
            g = jnp.dot(x, w_gate[:, n : n + wide_f], preferred_element_type=f32)
            u = jnp.dot(x, w_up[:, n : n + wide_f], preferred_element_type=f32)
            hid[0:size, n : n + wide_f] = (jax.nn.silu(g) * u).astype(bf16)
        for n in range(0, model, wide_f):
            y = jnp.dot(hid[0:size, :], w_down[:, n : n + wide_f], preferred_element_type=f32)
            put(n, y.astype(bf16))

    group = 4 if 4 * others * piece <= 512 else 1
    size = group * others * piece

    def experts_of(k):
        def run(m, _):
            block = pl.ds(m * group, group)

            def put(n, y):
                part[k, block, :, :, n : n + wide_f] = y.reshape(group, others, piece, wide_f)

            ffn(size, lambda: rows[k, block].reshape(size, model), put)
            return 0

        if group == 4:
            run(0, 0)
        else:
            lax.fori_loop(0, 4 // group, run, 0)

    def arrive(k):
        across(lambda j: z_got(k, j).wait_recv())
        x_copy(k).start()
        b_copy(k).start()

    half = model // 2

    def near_total(n, h, put):
        near_sum(n, h).wait_recv()
        for c in range(2):
            q = slice(c * half, (c + 1) * half)
            total = part_n[n, h, lo, :, q].astype(f32) + sum_in_n[n, h, :, q].astype(f32)
            put(c, total.astype(bf16))

    def near_expert(h):
        near_share(h).wait_recv()

        def put(n, y):
            part_n[1, h, :, :, n : n + wide_f] = y.reshape(2, slots, wide_f)

        ffn(2 * slots, lambda: rows_n[1, h].reshape(2 * slots, model), put)
        near_sum(1, h).start()

    def near_home(h):
        def put(c, y):
            total_n[h, c] = y
            near_return(h, c).start()

        near_total(1, h, put)

    dims = (((0,), (0,)), ((), ()))

    def near_combine(h, c, put):
        near_return(h, c).wait_recv()
        for n in range(0, half, wide):
            y = lax.dot_general(
                picks_n[h], near_back[h, c, :, :, n : n + wide].reshape(2 * slots, wide), dims, preferred_element_type=f32
            )
            put(n, y[0:count, :] + y[count:, :])

    def far_combine(c):
        def put(n, y):
            dense_send[c, :, n : n + wide] = y.astype(bf16)

        near_combine(1 - hi, c, put)
        dense_copy(c).start()

    def give_back(k):
        across(lambda i: r3_got(k, i).wait_recv())
        for n in range(0, model, wide):
            y = lax.dot_general(
                picks[k].reshape(others * piece, 2 * count), back[k, :, :, n : n + wide].reshape(others * piece, wide),
                dims, preferred_element_type=f32,
            )
            own[:, n : n + wide] = own[:, n : n + wide] + y[0:count, :] + y[count:, :]

    arrive(0)
    for c in dense:
        c.wait_recv()
    for n in range(0, model, wide):
        y = jnp.dot(onehot_n[...], hidden_far[:, n : n + wide], preferred_element_type=f32).astype(bf16)
        rows_n[0, 1 - hi, lo, :, n : n + wide] = y[0:slots, :]
        pack_n[1 - hi, :, n : n + wide] = y[slots:, :]
    near_far().start()
    for k in range(held, pieces):
        across(lambda i: z_out(k, i).start())
    local_copy(1 - hi).start()
    if pieces > 1:
        arrive(1)

    def put_local(n, y):
        part_n[0, :, :, :, n : n + wide_f] = y.reshape(2, 2, slots, wide_f)

    def local_expert():
        local_copy(hi).wait_recv()
        local_copy(1 - hi).wait_recv()
        ffn(4 * slots, lambda: rows_n[0].reshape(4 * slots, model), put_local)
        near_sum(0, 0).start()
        near_sum(0, 1).start()

    steps = {
        "share_own": 1, "expert_own": 2, "home_own": 3, "share": 3, "expert": 3, "home": 4, "local": 4, "total": 5, "cross": 6, "cross2": 6
    }
    turns = max(pieces + 3, max(steps.values()) + 1)

    def turn(d, _):
        def at(name, run):
            @pl.when(d == steps[name])
            def _():
                run()

        @pl.when(d < pieces + 1)
        def _():
            k = d - 1
            x_copy(k).wait_recv()
            c_copy(k).start()

        @pl.when(jnp.logical_and(d >= 2, d < pieces + 2))
        def _():
            k = d - 2
            r1_copy(k).wait_recv()

            def add(j):
                total = part[k, other, j].astype(f32) + sum_in[k, 1 - hi, j].astype(f32)
                sum_send[k, j] = total.astype(bf16)

            across(add)
            r2_copy(k).start()

        at("home_own", lambda: near_home(hi))
        at("home", lambda: near_home(1 - hi))
        @pl.when(jnp.logical_and(d >= 3, d < pieces + 3))
        def _():
            k = d - 3
            r2_copy(k).wait_recv()

            def add(j):
                total = part[k, mine, j].astype(f32) + sum_in[k, hi, j].astype(f32) + cross_in[k, j].astype(f32)
                done_out[k, j] = total.astype(bf16)

            across(add)
            across(lambda j: r3_copy(k, j).start())

        if pieces > 2:
            @pl.when(d == 1)
            def _():
                arrive(2)

        at("expert_own", lambda: near_expert(hi))

        def share():
            near_far().wait_recv()
            near_share(1 - hi).start()

        def share_own():
            for stage in stages:
                near_own(*stage).wait_recv()
            near_share(hi).start()

        at("share", share)

        @pl.when(d < pieces + 1)
        def _():
            k = d - 1
            b_copy(k).wait_recv()
            c_copy(k).wait_recv()
            experts_of(k)
            r1_copy(k).start()

        @pl.when(jnp.logical_and(d >= 2, d < pieces - 1))
        def _():
            arrive(d + 1)

        at("share_own", share_own)

        def total_local():
            for h in range(2):
                def put(c, y):
                    near_back[h, c, 0] = y

                near_total(0, h, put)

        at("expert", lambda: near_expert(1 - hi))
        at("local", local_expert)
        at("total", total_local)
        at("cross", lambda: far_combine(0))
        at("cross2", lambda: far_combine(1))
        return 0

    lax.fori_loop(1, turns, turn, 0)
    for k in range(max(pieces - 1, 0)):
        give_back(k)
    for c in range(2):
        def put(n, y):
            q = slice(c * half + n, c * half + n + wide)
            own[:, q] = own[:, q] + y

        near_combine(hi, c, put)
    for k in range(max(pieces - 1, 0), pieces):
        give_back(k)
    for c in range(2):
        dense_copy(c).wait_recv()

    finals = []
    for j in range(CHUNKS):
        q = slice(j * step, (j + 1) * step)
        crossed = jnp.concatenate([dense_in[0, q, :], dense_in[1, q, :]], axis=1).astype(f32)
        out[q, :] = layer_norm(own[q, :] + crossed, gain2[...], bias2[...]).astype(bf16)
        c = pltpu.make_async_copy(out.at[pl.ds(j * step, step)], out_h.at[pl.ds(j * step, step)], outs.at[j])
        c.start()
        finals.append(c)

    @pl.when(s < experts - 1)
    def _():
        for c in edges:
            c.wait_send()

    for c in beside + over + dense + swaps + [last, near_far()] + [near_own(*stage) for stage in stages]:
        c.wait_send()
    for h in range(2):
        for c in (local_copy(h), near_share(h), near_sum(0, h), near_sum(1, h), near_return(h, 0), near_return(h, 1), dense_copy(h)):
            c.wait_send()

    def drain(k):
        for c in (x_copy, b_copy, c_copy, r1_copy, r2_copy):
            c(k).wait_send()
        across(lambda i: z_out(k, i).wait_send())
        across(lambda j: r3_copy(k, j).wait_send())

    each(pieces, drain)
    for c in finals:
        c.wait()


def shards(
    gate_in, mult_in, value_in, doc_ids, conv_taps, out_proj, resid, norm1_gain, norm1_bias,
    expert_ids, expert_wts, w_gate, w_up, w_down, norm2_gain, norm2_bias,
):
    experts, parts = lax.axis_size("sp"), lax.axis_size("tp")
    assert parts == 4
    length, channels = mult_in.shape
    count, model = resid.shape
    top = expert_ids.shape[1]
    units = w_gate.shape[2]
    capacity = 5 * count * top // (4 * experts)
    piece = 16
    pieces = -(-capacity // piece)
    slots = pieces * piece
    padded = max(8, experts)
    others = experts - 2
    assert experts >= 4 and experts % 2 == 0
    hbm = pl.BlockSpec(memory_space=pl.ANY)
    V = pltpu.VMEM
    sems = pltpu.SemaphoreType.DMA
    blocks = (pieces, others, piece, model)
    routed = (pieces, 4, others, piece, model)
    batch = 4 * others * piece if 4 * others * piece <= 512 else others * piece
    batch = max(batch, 4 * slots)
    many, each_way = sems((pieces,)), sems((pieces, others))
    two, four = sems((2,)), sems((2, 2))
    return pl.pallas_call(
        functools.partial(kernel, experts, slots, piece),
        out_shape=jax.ShapeDtypeStruct((count, model), bf16),
        in_specs=[hbm] * 16,
        out_specs=hbm,
        scratch_shapes=[
            V((length, channels), bf16), V((length, channels), bf16), V((length, channels), bf16),
            V((1, length + 128), jnp.int32), V(conv_taps.shape, bf16), V((channels, model), bf16), V((count, model), bf16),
            V((1, model), f32), V((1, model), f32), V((top, count), jnp.int32), V((top, count), f32),
            V((model, units), bf16), V((model, units), bf16), V((units, model), bf16), V((1, model), f32), V((1, model), f32),
            V((16, channels), bf16), V((16, channels), bf16),
            V((length + 8, channels), f32), V((length + 8, 128), f32), V((length, channels), bf16),
            V((2, count, model), bf16), V((2, count, model), bf16), V((count, model), bf16), V((count, model), bf16),
            V((count, model), f32), V((count, model), bf16), V((count, model), bf16), V((count, model), bf16),
            V((top, count), jnp.int32), V((top, count), f32),
            V((2, padded, count), f32), V((2, padded, count), f32), V((2 * slots, count), bf16),
            V((pieces, experts, piece, count), bf16), V((2, 2 * slots, 2 * count), bf16), V((pieces, others, piece, 2 * count), bf16),
            V((2, 2, 2, slots, model), bf16), V((2, 2, 2, slots, model), bf16), V((2, slots, model), bf16),
            V((2, 2, slots, model), bf16), V((2, 2, slots, model // 2), bf16), V((2, 2, 2, slots, model // 2), bf16),
            V((2, count, model // 2), bf16), V((2, count, model // 2), bf16),
            V(blocks, bf16), V(routed, bf16), V(routed, bf16), V((batch, units), bf16),
            V((pieces, 2, others, piece, model), bf16), V(blocks, bf16), V(blocks, bf16), V(blocks, bf16),
            V(blocks, bf16),
            sems((16,)), sems((CHUNKS,)), sems((3,)), sems((3,)), sems((2 * CHUNKS + 1,)), sems((2 * CHUNKS + 1,)),
            two, two, sems((CHUNKS,)), sems((CHUNKS,)),
            two, two, sems((CHUNKS + 1,)), sems((CHUNKS + 1,)), two, two, four, four, four, four, two, two,
            each_way, each_way, many, many, many, many, many, many,
            many, many, many, many, each_way, each_way,
        ],
        compiler_params=pltpu.CompilerParams(
            collective_id=0, has_side_effects=True, vmem_limit_bytes=62 * 2**20
        ),
    )(
        gate_in, mult_in, value_in, doc_ids[None], conv_taps, out_proj, resid,
        norm1_gain[None], norm1_bias[None], expert_ids.T, expert_wts.T,
        w_gate[0], w_up[0], w_down[0], norm2_gain[None], norm2_bias[None],
    )


def solution(mesh):
    placed = (
        P(("grp", "sp"), "tp"),
        P(("grp", "sp"), "tp"),
        P(("grp", "sp"), "tp"),
        P(("grp", "sp")),
        P(None, "tp"),
        P("tp", None),
        P(("grp", "sp", "tp"), None),
        P(),
        P(),
        P(("grp", "sp", "tp"), None),
        P(("grp", "sp", "tp"), None),
        P("sp", None, "tp"),
        P("sp", None, "tp"),
        P("sp", "tp", None),
        P(),
        P(),
    )
    return jax.shard_map(
        shards, mesh=mesh, in_specs=placed, out_specs=P(("grp", "sp", "tp"), None), check_vma=False
    )
```

```python
import functools

import jax
import jax.numpy as jnp
from jax import lax
from jax.experimental import pallas as pl
from jax.experimental.pallas import tpu as pltpu
from jax.sharding import PartitionSpec as P

residual_scale = 2.0**0.5
norm_eps = 1e-05
MESH = pl.DeviceIdType.MESH
f32, bf16 = jnp.float32, jnp.bfloat16
CHUNKS = 4


def layer_norm(pre, gain, bias):
    center = pre - jnp.mean(pre, axis=-1, keepdims=True)
    spread = jnp.mean(center * center, axis=-1, keepdims=True)
    return center * lax.rsqrt(spread + norm_eps) * gain + bias


def remote(src, dst, send, recv, **where):
    return pltpu.make_async_remote_copy(
        src_ref=src, dst_ref=dst, send_sem=send, recv_sem=recv, device_id=where, device_id_type=MESH
    )


def kernel(
    experts, slots, piece,
    gate_h, mult_h, value_h, docs_h, taps_h, proj_h, resid_h, gain1_h, bias1_h, ids_h, wts_h,
    w_gate_h, w_up_h, w_down_h, gain2_h, bias2_h,
    out_h,
    gate, mult, value, docs, taps, proj, resid, gain1, bias1, ids, wts, w_gate, w_up, w_down, gain2, bias2,
    edge_m, edge_v, ext, ext_docs, heads,
    send1, got1, send2, got2, own, hidden, hidden_far, out, ids_far, wts_far,
    slot_of, weight_of, onehot_n, onehot, picks_n, picks,
    rows_n, part_n, pack_n, sum_in_n, total_n, near_back, dense_send, dense_in,
    packed, rows, part, hid, sum_in, sum_send, cross_in, done_out, back,
    local, outs, edge_s, edge_r, mix_s, mix_r, swap_s, swap_r, dense_s, dense_r,
    lbs, lbr, ns, nr, nbs, nbr, n1s, n1r, rns, rnr, des, der,
    zs, zr, xs, xr, bs, br, cs, cr, r1s, r1r, r2s, r2r, r3s, r3r,
):
    s, t = lax.axis_index("sp"), lax.axis_index("tp")
    hi, lo = t // 2, t % 2
    sib, far = hi * 2 + (1 - lo), (1 - hi) * 2 + lo
    count, model = resid.shape
    length, channels = mult.shape
    taps_n = taps.shape[0]
    top = ids.shape[0]
    others = experts - 2
    pieces = slots // piece
    parity = s % 2
    base = s - parity
    near = base + 1 - parity

    def load(i, a, b):
        return pltpu.make_async_copy(a, b, local.at[i])

    pairs = [
        (mult_h, mult), (value_h, value), (docs_h, docs.at[:, 128 : 128 + length]), (taps_h, taps), (gate_h, gate),
        (proj_h, proj), (resid_h, resid), (gain1_h, gain1), (bias1_h, bias1), (ids_h, ids), (wts_h, wts),
        (w_gate_h, w_gate), (w_up_h, w_up), (w_down_h, w_down), (gain2_h, gain2), (bias2_h, bias2),
    ]
    loads = [load(i, a, b) for i, (a, b) in enumerate(pairs)]
    for c in loads[:11]:
        c.start()

    barrier = pltpu.get_barrier_semaphore()

    def greet(d, _):
        pl.semaphore_signal(barrier, inc=1, device_id={"sp": (s + d) % experts}, device_id_type=MESH)
        return 0

    lax.fori_loop(1, experts, greet, 0)
    pl.semaphore_signal(barrier, inc=1, device_id={"tp": sib}, device_id_type=MESH)
    pl.semaphore_signal(barrier, inc=1, device_id={"tp": far}, device_id_type=MESH)
    for c in loads[:3]:
        c.wait()
    pl.semaphore_wait(barrier, experts + 1)

    nxt = (s + 1) % experts
    edges = [
        remote(mult.at[pl.ds(length - 16, 16)], edge_m, edge_s.at[0], edge_r.at[0], sp=nxt),
        remote(value.at[pl.ds(length - 16, 16)], edge_v, edge_s.at[1], edge_r.at[1], sp=nxt),
        remote(docs.at[:, pl.ds(length, 128)], docs.at[:, pl.ds(0, 128)], edge_s.at[2], edge_r.at[2], sp=nxt),
    ]

    @pl.when(s < experts - 1)
    def _():
        for c in edges:
            c.start()

    for c in loads[11:]:
        c.start()

    ones = jnp.ones((128, 128), bf16)
    row_no = lax.broadcasted_iota(jnp.int32, (128, 128), 0)
    lane_no = lax.broadcasted_iota(jnp.int32, (128, 128), 1)

    def column(line, shift, height):
        spread = jnp.where(row_no[:height] + shift == lane_no[:height], line.astype(f32), 0.0)
        return jnp.dot(spread.astype(bf16), ones, preferred_element_type=f32)

    for r in range(0, length, 128):
        ext[8 + r : 8 + r + 128, :] = mult[r : r + 128, :].astype(f32) * value[r : r + 128, :].astype(f32)
        ext_docs[8 + r : 8 + r + 128, :] = column(docs[:, 128 + r : 256 + r], 0, 128)
    ext[0:8, :] = jnp.zeros((8, channels), f32)
    ext_docs[0:8, :] = jnp.full((8, 128), -1.0, f32)
    for c in loads[3:5]:
        c.wait()

    def convolve(r, height):
        now = ext_docs[8 + r : 8 + r + height, :]
        same = [ext_docs[8 + r - b : 8 + r - b + height, :] == now for b in range(1, taps_n)]
        for c in range(0, channels, 128):
            tap = taps[:, c : c + 128].astype(f32)
            acc = tap[taps_n - 1 :] * ext[8 + r : 8 + r + height, c : c + 128]
            for b in range(1, taps_n):
                moved = ext[8 + r - b : 8 + r - b + height, c : c + 128]
                acc = acc + tap[taps_n - 1 - b : taps_n - b] * jnp.where(same[b - 1], moved, 0.0)
            heads[r : r + height, c : c + 128] = (gate[r : r + height, c : c + 128].astype(f32) * acc).astype(bf16)

    for r in range(0, length, 64):
        convolve(r, 64)

    @pl.when(s > 0)
    def _():
        for c in edges:
            c.wait_recv()
        ext[0:8, :] = (edge_m[...].astype(f32) * edge_v[...].astype(f32))[8:16, :]
        ext_docs[0:8, :] = column(docs[:, 0:128], 120, 8)
        convolve(0, 16)

    for c in loads[7:11]:
        c.wait()
    swaps = [
        remote(ids, ids_far, swap_s.at[0], swap_r.at[0], tp=far),
        remote(wts, wts_far, swap_s.at[1], swap_r.at[1], tp=far),
    ]
    for c in swaps:
        c.start()
    loads[5].wait()
    wide = 512

    def projected(number, n):
        return jnp.dot(
            heads[pl.ds(pl.multiple_of(number * count, count), count), :], proj[:, n : n + wide],
            preferred_element_type=f32,
        )

    step = count // CHUNKS
    beside = [
        remote(send1.at[0, pl.ds(j * step, step)], got1.at[0, pl.ds(j * step, step)], mix_s.at[j], mix_r.at[j], tp=sib)
        for j in range(CHUNKS)
    ]
    over = [
        remote(send2.at[pl.ds(j * step, step)], got2.at[pl.ds(j * step, step)], mix_s.at[CHUNKS + j], mix_r.at[CHUNKS + j], tp=far)
        for j in range(CHUNKS)
    ]
    last = remote(send1.at[1], got1.at[1], mix_s.at[2 * CHUNKS], mix_r.at[2 * CHUNKS], tp=sib)
    dense = [
        remote(hidden.at[pl.ds(j * step, step)], hidden_far.at[pl.ds(j * step, step)], dense_s.at[j], dense_r.at[j], tp=far)
        for j in range(CHUNKS)
    ]
    for n in range(0, model, wide):
        send1[0, :, n : n + wide] = projected((1 - hi) * 2 + (1 - lo), n).astype(bf16)
    for c in beside:
        c.start()
    for n in range(0, model, wide):
        own[:, n : n + wide] = projected((1 - hi) * 2 + lo, n)
    for j in range(CHUNKS):
        q = slice(j * step, (j + 1) * step)
        beside[j].wait_recv()
        send2[q, :] = (own[q, :] + got1[0, q, :].astype(f32)).astype(bf16)
        over[j].start()
    for n in range(0, model, wide):
        send1[1, :, n : n + wide] = projected(hi * 2 + (1 - lo), n).astype(bf16)
    last.start()
    loads[6].wait()
    for n in range(0, model, wide):
        own[:, n : n + wide] = projected(t, n) + residual_scale * resid[:, n : n + wide].astype(f32)
    last.wait_recv()
    for n in range(0, model, wide):
        own[:, n : n + wide] = own[:, n : n + wide] + got1[1, :, n : n + wide].astype(f32)

    padded = slot_of.shape[1]
    expert_no = lax.broadcasted_iota(jnp.int32, (padded, count), 0)
    token_no = lax.broadcasted_iota(jnp.int32, (padded, count), 1)
    before = lax.broadcasted_iota(jnp.int32, (count, count), 0) < lax.broadcasted_iota(
        jnp.int32, (count, count), 1
    )
    slot_no = lax.broadcasted_iota(jnp.int32, (slots, count), 0).astype(f32)
    ready = [max(0, slots - (count - (j + 1) * step)) // piece for j in range(CHUNKS)]

    def choose(side, e, put):
        selected = slot_no == slot_of[side, pl.ds(e, 1), :]
        pick = jnp.where(selected, weight_of[side, pl.ds(e, 1), :], 0.0)
        high = pick.astype(bf16)
        put(jnp.where(selected, 1.0, 0.0).astype(bf16), high, (pick - high.astype(f32)).astype(bf16))

    def route(side, own_side, its_ids, its_wts):
        chosen = jnp.zeros((padded, count), f32)
        weight = jnp.zeros((padded, count), f32)
        for k in range(top):
            same = its_ids[k : k + 1, :] == expert_no
            chosen = chosen + jnp.where(same, 1.0, 0.0)
            weight = weight + jnp.where(same, its_wts[k : k + 1, :], 0.0)
        rank = jnp.dot(chosen.astype(bf16), jnp.where(before, 1.0, 0.0).astype(bf16), preferred_element_type=f32)
        slot, placed, open_ = jnp.full((padded, count), -1.0, f32), jnp.zeros((padded, 1), f32), 0
        for j in range(CHUNKS):
            seen = jnp.where(token_no < (j + 1) * step, chosen, 0.0)
            upto = jnp.minimum(jnp.sum(seen, axis=1, keepdims=True), placed + float(ready[j] * piece - open_))
            here = jnp.logical_and(rank >= placed, rank < upto)
            slot = jnp.where(here, rank - placed + float(open_), slot)
            placed, open_ = upto, ready[j] * piece
        slot_of[side] = jnp.where(chosen > 0.5, slot, -1.0)
        weight_of[side] = weight
        for n, e in enumerate((s, near)):
            def put(one, high, low):
                if own_side:
                    for k in range(pieces):
                        onehot[k, others + n] = one[k * piece : (k + 1) * piece, :]
                else:
                    onehot_n[n * slots : (n + 1) * slots, :] = one
                picks_n[side, n * slots : (n + 1) * slots, 0:count] = high
                picks_n[side, n * slots : (n + 1) * slots, count : 2 * count] = low

            choose(side, e, put)

    route(hi, True, ids, wts)

    def choose_step(i, _):
        def put(one, high, low):
            for k in range(pieces):
                onehot[k, i] = one[k * piece : (k + 1) * piece, :]
                picks[k, i, :, 0:count] = high[k * piece : (k + 1) * piece, :]
                picks[k, i, :, count : 2 * count] = low[k * piece : (k + 1) * piece, :]

        choose(hi, (base + 2 + i) % experts, put)
        return 0

    lax.fori_loop(0, others, choose_step, 0)
    for c in swaps:
        c.wait_recv()
    route(1 - hi, False, ids_far, wts_far)

    hidden[...] = jnp.zeros((count, model), bf16)

    mine, other = lo * 2 + hi, lo * 2 + 1 - hi

    def z_out(k, i):
        j = 2 * (i // 2) + parity
        return remote(packed.at[k, i], rows.at[k, mine, j], zs.at[k, i], zr.at[k, j], sp=(base + 2 + i) % experts)

    def z_got(k, j):
        return remote(packed.at[k, j], rows.at[k, mine, j], zs.at[k, j], zr.at[k, j], sp=near)

    def x_copy(k):
        block = rows.at[k, mine]
        return remote(block, block, xs.at[k], xr.at[k], tp=far)

    def b_copy(k):
        block = rows.at[k, mine]
        return remote(block, block, bs.at[k], br.at[k], tp=sib)

    def c_copy(k):
        block = rows.at[k, other]
        return remote(block, block, cs.at[k], cr.at[k], tp=sib)

    def r1_copy(k):
        return remote(part.at[k, pl.ds((1 - lo) * 2, 2)], sum_in.at[k], r1s.at[k], r1r.at[k], tp=sib)

    def r2_copy(k):
        return remote(sum_send.at[k], cross_in.at[k], r2s.at[k], r2r.at[k], tp=far)

    def r3_copy(k, j):
        i = 2 * (j // 2) + parity
        to = (base - 2 - 2 * (j // 2) + j % 2 + experts) % experts
        return remote(done_out.at[k, j], back.at[k, i], r3s.at[k, j], r3r.at[k, i], sp=to)

    def r3_got(k, i):
        return remote(done_out.at[k, i], back.at[k, i], r3s.at[k, i], r3r.at[k, i], sp=near)

    def local_copy(h):
        block = rows_n.at[0, h, lo]
        return remote(block, block, lbs.at[h], lbr.at[h], tp=sib)

    def near_far():
        return remote(pack_n.at[1 - hi], rows_n.at[1, 1 - hi, lo], ns.at[CHUNKS], nr.at[CHUNKS], sp=near)

    def near_own(j, first, stop):
        q = pl.ds(first * piece, (stop - first) * piece)
        return remote(pack_n.at[hi, q], rows_n.at[1, hi, lo, q], ns.at[j], nr.at[j], sp=near)

    stages, begun = [], 0
    for j in range(CHUNKS):
        if ready[j] > begun:
            stages.append((j, begun, ready[j]))
            begun = ready[j]
    held = max(pieces - 1, 1)

    def near_share(h):
        block = rows_n.at[1, h, lo]
        return remote(block, block, nbs.at[h], nbr.at[h], tp=sib)

    def near_sum(n, h):
        return remote(part_n.at[n, h, 1 - lo], sum_in_n.at[n, h], n1s.at[n, h], n1r.at[n, h], tp=sib)

    def near_return(h, c):
        return remote(total_n.at[h, c], near_back.at[h, c, 1], rns.at[h, c], rnr.at[h, c], sp=near)

    def dense_copy(c):
        return remote(dense_send.at[c], dense_in.at[c], des.at[c], der.at[c], tp=far)

    def each(count_of, run):
        def step(i, _):
            run(i)
            return 0

        lax.fori_loop(0, count_of, step, 0)

    def across(run):
        each(others, run)

    for j in range(CHUNKS):
        over[j].wait_recv()
        q = slice(j * step, (j + 1) * step)
        hidden[q, :] = layer_norm(own[q, :] + got2[q, :].astype(f32), gain1[...], bias1[...]).astype(bf16)
        dense[j].start()
        for number, first, stop in stages:
            if number != j:
                continue
            span = stop - first
            q = slice(first * piece, stop * piece)
            for n in range(0, model, wide):
                y = jnp.dot(
                    onehot[first:stop].reshape(span * experts * piece, count), hidden[:, n : n + wide],
                    preferred_element_type=f32,
                ).astype(bf16).reshape(span, experts, piece, wide)
                packed[first:stop, :, :, n : n + wide] = y[:, :others]
                rows_n[0, hi, lo, q, n : n + wide] = y[:, others].reshape(span * piece, wide)
                pack_n[hi, q, n : n + wide] = y[:, others + 1].reshape(span * piece, wide)
            near_own(j, first, stop).start()
            for k in range(first, min(stop, held)):
                across(lambda i: z_out(k, i).start())

    local_copy(hi).start()
    for n in range(0, model, wide):
        own[:, n : n + wide] = residual_scale * hidden[:, n : n + wide].astype(f32)
    for c in loads[11:]:
        c.wait()

    wide_f = 256

    def ffn(size, take, put):
        for n in range(0, w_gate.shape[1], wide_f):
            x = take()
            g = jnp.dot(x, w_gate[:, n : n + wide_f], preferred_element_type=f32)
            u = jnp.dot(x, w_up[:, n : n + wide_f], preferred_element_type=f32)
            hid[0:size, n : n + wide_f] = (jax.nn.silu(g) * u).astype(bf16)
        for n in range(0, model, wide_f):
            y = jnp.dot(hid[0:size, :], w_down[:, n : n + wide_f], preferred_element_type=f32)
            put(n, y.astype(bf16))

    group = 4 if 4 * others * piece <= 512 else 1
    size = group * others * piece

    def experts_of(k):
        def run(m, _):
            block = pl.ds(m * group, group)

            def put(n, y):
                part[k, block, :, :, n : n + wide_f] = y.reshape(group, others, piece, wide_f)

            ffn(size, lambda: rows[k, block].reshape(size, model), put)
            return 0

        if group == 4:
            run(0, 0)
        else:
            lax.fori_loop(0, 4 // group, run, 0)

    def arrive(k):
        across(lambda j: z_got(k, j).wait_recv())
        x_copy(k).start()
        b_copy(k).start()

    half = model // 2

    def near_total(n, h, put):
        near_sum(n, h).wait_recv()
        for c in range(2):
            q = slice(c * half, (c + 1) * half)
            total = part_n[n, h, lo, :, q].astype(f32) + sum_in_n[n, h, :, q].astype(f32)
            put(c, total.astype(bf16))

    def near_expert(h):
        near_share(h).wait_recv()

        def put(n, y):
            part_n[1, h, :, :, n : n + wide_f] = y.reshape(2, slots, wide_f)

        ffn(2 * slots, lambda: rows_n[1, h].reshape(2 * slots, model), put)
        near_sum(1, h).start()

    def near_home(h):
        def put(c, y):
            total_n[h, c] = y
            near_return(h, c).start()

        near_total(1, h, put)

    dims = (((0,), (0,)), ((), ()))

    def near_combine(h, c, put):
        near_return(h, c).wait_recv()
        for n in range(0, half, wide):
            y = lax.dot_general(
                picks_n[h], near_back[h, c, :, :, n : n + wide].reshape(2 * slots, wide), dims, preferred_element_type=f32
            )
            put(n, y[0:count, :] + y[count:, :])

    def far_combine(c):
        def put(n, y):
            dense_send[c, :, n : n + wide] = y.astype(bf16)

        near_combine(1 - hi, c, put)
        dense_copy(c).start()

    def give_back(k):
        across(lambda i: r3_got(k, i).wait_recv())
        for n in range(0, model, wide):
            y = lax.dot_general(
                picks[k].reshape(others * piece, 2 * count), back[k, :, :, n : n + wide].reshape(others * piece, wide),
                dims, preferred_element_type=f32,
            )
            own[:, n : n + wide] = own[:, n : n + wide] + y[0:count, :] + y[count:, :]

    arrive(0)
    for c in dense:
        c.wait_recv()
    for n in range(0, model, wide):
        y = jnp.dot(onehot_n[...], hidden_far[:, n : n + wide], preferred_element_type=f32).astype(bf16)
        rows_n[0, 1 - hi, lo, :, n : n + wide] = y[0:slots, :]
        pack_n[1 - hi, :, n : n + wide] = y[slots:, :]
    near_far().start()
    for k in range(held, pieces):
        across(lambda i: z_out(k, i).start())
    local_copy(1 - hi).start()
    if pieces > 1:
        arrive(1)

    def put_local(n, y):
        part_n[0, :, :, :, n : n + wide_f] = y.reshape(2, 2, slots, wide_f)

    def local_expert():
        local_copy(hi).wait_recv()
        local_copy(1 - hi).wait_recv()
        ffn(4 * slots, lambda: rows_n[0].reshape(4 * slots, model), put_local)
        near_sum(0, 0).start()
        near_sum(0, 1).start()

    steps = {
        "share_own": 1, "expert_own": 2, "home_own": 3, "share": 3, "expert": 3, "home": 4, "local": 4, "total": 5, "cross": 6, "cross2": 6
    }
    turns = max(pieces + 3, max(steps.values()) + 1)

    def turn(d, _):
        def at(name, run):
            @pl.when(d == steps[name])
            def _():
                run()

        @pl.when(d < pieces + 1)
        def _():
            k = d - 1
            x_copy(k).wait_recv()
            c_copy(k).start()

        @pl.when(jnp.logical_and(d >= 2, d < pieces + 2))
        def _():
            k = d - 2
            r1_copy(k).wait_recv()

            def add(j):
                total = part[k, other, j].astype(f32) + sum_in[k, 1 - hi, j].astype(f32)
                sum_send[k, j] = total.astype(bf16)

            across(add)
            r2_copy(k).start()

        at("home_own", lambda: near_home(hi))
        at("home", lambda: near_home(1 - hi))
        @pl.when(jnp.logical_and(d >= 3, d < pieces + 3))
        def _():
            k = d - 3
            r2_copy(k).wait_recv()

            def add(j):
                total = part[k, mine, j].astype(f32) + sum_in[k, hi, j].astype(f32) + cross_in[k, j].astype(f32)
                done_out[k, j] = total.astype(bf16)

            across(add)
            across(lambda j: r3_copy(k, j).start())

        if pieces > 2:
            @pl.when(d == 1)
            def _():
                arrive(2)

        at("expert_own", lambda: near_expert(hi))

        def share():
            near_far().wait_recv()
            near_share(1 - hi).start()

        def share_own():
            for stage in stages:
                near_own(*stage).wait_recv()
            near_share(hi).start()

        at("share", share)

        @pl.when(d < pieces + 1)
        def _():
            k = d - 1
            b_copy(k).wait_recv()
            c_copy(k).wait_recv()
            experts_of(k)
            r1_copy(k).start()

        @pl.when(jnp.logical_and(d >= 2, d < pieces - 1))
        def _():
            arrive(d + 1)

        at("share_own", share_own)

        def total_local():
            for h in range(2):
                def put(c, y):
                    near_back[h, c, 0] = y

                near_total(0, h, put)

        at("expert", lambda: near_expert(1 - hi))
        at("local", local_expert)
        at("total", total_local)
        at("cross", lambda: far_combine(0))
        at("cross2", lambda: far_combine(1))
        return 0

    lax.fori_loop(1, turns, turn, 0)
    for k in range(max(pieces - 1, 0)):
        give_back(k)
    for c in range(2):
        def put(n, y):
            q = slice(c * half + n, c * half + n + wide)
            own[:, q] = own[:, q] + y

        near_combine(hi, c, put)
    for c in range(2):
        dense_copy(c).wait_recv()
        q = slice(c * half, (c + 1) * half)
        own[:, q] = own[:, q] + dense_in[c].astype(f32)
    give_back(pieces - 1)

    finals = []
    for j in range(CHUNKS):
        q = slice(j * step, (j + 1) * step)
        out[q, :] = layer_norm(own[q, :], gain2[...], bias2[...]).astype(bf16)
        c = pltpu.make_async_copy(out.at[pl.ds(j * step, step)], out_h.at[pl.ds(j * step, step)], outs.at[j])
        c.start()
        finals.append(c)

    @pl.when(s < experts - 1)
    def _():
        for c in edges:
            c.wait_send()

    for c in beside + over + dense + swaps + [last, near_far()] + [near_own(*stage) for stage in stages]:
        c.wait_send()
    for h in range(2):
        for c in (local_copy(h), near_share(h), near_sum(0, h), near_sum(1, h), near_return(h, 0), near_return(h, 1), dense_copy(h)):
            c.wait_send()

    def drain(k):
        for c in (x_copy, b_copy, c_copy, r1_copy, r2_copy):
            c(k).wait_send()
        across(lambda i: z_out(k, i).wait_send())
        across(lambda j: r3_copy(k, j).wait_send())

    each(pieces, drain)
    for c in finals:
        c.wait()


def shards(
    gate_in, mult_in, value_in, doc_ids, conv_taps, out_proj, resid, norm1_gain, norm1_bias,
    expert_ids, expert_wts, w_gate, w_up, w_down, norm2_gain, norm2_bias,
):
    experts, parts = lax.axis_size("sp"), lax.axis_size("tp")
    assert parts == 4
    length, channels = mult_in.shape
    count, model = resid.shape
    top = expert_ids.shape[1]
    units = w_gate.shape[2]
    capacity = 5 * count * top // (4 * experts)
    piece = 16
    pieces = -(-capacity // piece)
    slots = pieces * piece
    padded = max(8, experts)
    others = experts - 2
    assert experts >= 4 and experts % 2 == 0
    hbm = pl.BlockSpec(memory_space=pl.ANY)
    V = pltpu.VMEM
    sems = pltpu.SemaphoreType.DMA
    blocks = (pieces, others, piece, model)
    routed = (pieces, 4, others, piece, model)
    batch = 4 * others * piece if 4 * others * piece <= 512 else others * piece
    batch = max(batch, 4 * slots)
    many, each_way = sems((pieces,)), sems((pieces, others))
    two, four = sems((2,)), sems((2, 2))
    return pl.pallas_call(
        functools.partial(kernel, experts, slots, piece),
        out_shape=jax.ShapeDtypeStruct((count, model), bf16),
        in_specs=[hbm] * 16,
        out_specs=hbm,
        scratch_shapes=[
            V((length, channels), bf16), V((length, channels), bf16), V((length, channels), bf16),
            V((1, length + 128), jnp.int32), V(conv_taps.shape, bf16), V((channels, model), bf16), V((count, model), bf16),
            V((1, model), f32), V((1, model), f32), V((top, count), jnp.int32), V((top, count), f32),
            V((model, units), bf16), V((model, units), bf16), V((units, model), bf16), V((1, model), f32), V((1, model), f32),
            V((16, channels), bf16), V((16, channels), bf16),
            V((length + 8, channels), f32), V((length + 8, 128), f32), V((length, channels), bf16),
            V((2, count, model), bf16), V((2, count, model), bf16), V((count, model), bf16), V((count, model), bf16),
            V((count, model), f32), V((count, model), bf16), V((count, model), bf16), V((count, model), bf16),
            V((top, count), jnp.int32), V((top, count), f32),
            V((2, padded, count), f32), V((2, padded, count), f32), V((2 * slots, count), bf16),
            V((pieces, experts, piece, count), bf16), V((2, 2 * slots, 2 * count), bf16), V((pieces, others, piece, 2 * count), bf16),
            V((2, 2, 2, slots, model), bf16), V((2, 2, 2, slots, model), bf16), V((2, slots, model), bf16),
            V((2, 2, slots, model), bf16), V((2, 2, slots, model // 2), bf16), V((2, 2, 2, slots, model // 2), bf16),
            V((2, count, model // 2), bf16), V((2, count, model // 2), bf16),
            V(blocks, bf16), V(routed, bf16), V(routed, bf16), V((batch, units), bf16),
            V((pieces, 2, others, piece, model), bf16), V(blocks, bf16), V(blocks, bf16), V(blocks, bf16),
            V(blocks, bf16),
            sems((16,)), sems((CHUNKS,)), sems((3,)), sems((3,)), sems((2 * CHUNKS + 1,)), sems((2 * CHUNKS + 1,)),
            two, two, sems((CHUNKS,)), sems((CHUNKS,)),
            two, two, sems((CHUNKS + 1,)), sems((CHUNKS + 1,)), two, two, four, four, four, four, two, two,
            each_way, each_way, many, many, many, many, many, many,
            many, many, many, many, each_way, each_way,
        ],
        compiler_params=pltpu.CompilerParams(
            collective_id=0, has_side_effects=True, vmem_limit_bytes=62 * 2**20
        ),
    )(
        gate_in, mult_in, value_in, doc_ids[None], conv_taps, out_proj, resid,
        norm1_gain[None], norm1_bias[None], expert_ids.T, expert_wts.T,
        w_gate[0], w_up[0], w_down[0], norm2_gain[None], norm2_bias[None],
    )


def solution(mesh):
    placed = (
        P(("grp", "sp"), "tp"),
        P(("grp", "sp"), "tp"),
        P(("grp", "sp"), "tp"),
        P(("grp", "sp")),
        P(None, "tp"),
        P("tp", None),
        P(("grp", "sp", "tp"), None),
        P(),
        P(),
        P(("grp", "sp", "tp"), None),
        P(("grp", "sp", "tp"), None),
        P("sp", None, "tp"),
        P("sp", None, "tp"),
        P("sp", "tp", None),
        P(),
        P(),
    )
    return jax.shard_map(
        shards, mesh=mesh, in_specs=placed, out_specs=P(("grp", "sp", "tp"), None), check_vma=False
    )
```
